512 devices in a mesh: ep: 16 (over y, x), tp: 32 (over z, core).
Axes of the slice: x: 4, y: 4, z: 16, core: 2. Of those that a mesh axis runs over, the one named last changes fastest.
Arguments:
- tokens: bfloat16 [4096, 2048], P('ep'), may hold values from -6 to 6
- cotangent: bfloat16 [4096, 2048], P('ep'), may hold values from -6 to 6
- group_prob: float32 [4096], P('ep'), may hold values from 0.25 to 1
- expert_prob: float32 [4096, 2], P('ep'), may hold values from 0.1 to 1
- routing: int32 [4096, 2], P('ep'), may hold values from 0 to 15, all different within a row; in each aligned block of 256 rows (0 to 255, 256 to 511, ...) at most 48 rows name the same one
- gate_weight: bfloat16 [16, 2048, 4096], P('ep', None, 'tp'), may hold values from -0.125 to 0.125
- up_weight: bfloat16 [16, 2048, 4096], P('ep', None, 'tp'), may hold values from -0.125 to 0.125
- down_weight: bfloat16 [16, 4096, 2048], P('ep', 'tp'), may hold values from -1 to 1
Outputs:
- token_grad: bfloat16 [4096, 2048], P('ep')
- group_prob_grad: float32 [4096], P('ep')
- expert_prob_grad: float32 [4096, 2], P('ep')
- gate_weight_grad: bfloat16 [16, 2048, 4096], P('ep', None, 'tp')
- up_weight_grad: bfloat16 [16, 2048, 4096], P('ep', None, 'tp')
- down_weight_grad: bfloat16 [16, 4096, 2048], P('ep', 'tp')
- gate_row_norms: float32 [16, 2048], P('ep')
- up_row_norms: float32 [16, 2048], P('ep')
- down_row_norms: float32 [16, 4096], P('ep', 'tp')
The draws below stay inside these ranges and needn't reach their ends.
Inputs may be any that keep to these rules, and one draw needn't show every extreme that they name: `routing`: each row names 2 different experts. In each aligned block of 256 rows no expert is named by more than 48 rows, and in every draw some expert is named by exactly 48 rows of some block.
All inputs are finite; a program needn't handle non-finite values.
Results may differ from the reference program's by a relative error of at most 0.0065.
Values may be sent and summed in bfloat16 or wider, within the bound.
A program may use at most 64 MiB of HBM per device.

```python
import math
import jax
import jax.numpy as jnp
import numpy as np
from jax import lax

D = 2048
FF = 4096
TOP_K = 2
TOK_DEV = 256
EXPERTS = 16
CAP = 48
TOKENS = 4096
N_EP = 16


def draw_down_weight(key, part):
    first, second = jax.random.split(key, 2)
    base = jax.random.normal(first, (EXPERTS, FF, D), jnp.float32)
    rough = jax.random.uniform(second, (EXPERTS, FF, 1), jnp.float32, 0.0, 1.0)
    position = jnp.arange(FF, dtype=jnp.float32).reshape(1, FF, 1) / FF
    log_scale = jnp.log(10.0) * (rough - 0.5) + jnp.log(3.0) * (position - 0.5)
    scale = jnp.exp(log_scale)
    scale = scale / jnp.sqrt(jnp.mean(scale * scale, axis=1, keepdims=True))
    values = jnp.clip(base * scale * FF ** (-0.5), -1.0, 1.0)
    return values.astype(jnp.bfloat16)


def block_scale(rng, dims, cuts, smallest, largest):
    factor_of = 1.0
    for axis_at, parts in cuts:
        steps = jax.random.uniform(jax.random.fold_in(jax.random.fold_in(rng, 6), axis_at), (parts,), jnp.float32, smallest / len(cuts), largest / len(cuts))
        factor_of = factor_of * jnp.repeat(jnp.exp(steps), dims[axis_at] // parts).reshape((-1,) + (1,) * (len(dims) - 1 - axis_at))
    return factor_of


def assign_block(rng, own, number, rows, amount, top, bound, skew):
    ranking = jax.random.permutation(rng, amount)
    heavy_load, ordinary = portions_of(amount, rows * top, bound, skew, True), portions_of(amount, rows * top, bound, skew, False)
    places = jnp.arange(amount)

    def named(lengths, offset_by):
        used = int((lengths > 0).sum())
        fixed = max(1, used // 4)
        passed = fixed + (places - fixed + offset_by * (used - fixed)) % max(1, amount - fixed)
        return jnp.zeros((amount,), jnp.int32).at[ranking[jnp.where(places < fixed, places, passed)]].set(jnp.asarray(lengths, jnp.int32))

    lengths = jnp.where(number % 4 == 0, named(heavy_load, number // 4), named(ordinary, number - number // 4 - 1))
    mixed = jax.random.permutation(jax.random.fold_in(own, 3), amount)
    donor, sink = mixed[0:amount // 2 * 2:2], mixed[1:amount // 2 * 2:2]
    margin = jnp.minimum(lengths[donor] - 1, bound - lengths[sink]) // 2
    margin = jnp.where((donor == ranking[0]) | (sink == ranking[0]) | (lengths[sink] == 0), 0, jnp.maximum(margin, 0))
    passed = jax.random.randint(jax.random.fold_in(own, 4), (amount // 2,), 0, 1 << 20) % (margin + 1)
    lengths = lengths.at[donor].add(-passed).at[sink].add(passed)
    labels = jnp.searchsorted(jnp.cumsum(lengths), jnp.arange(rows * top), side="right").astype(jnp.int32)
    grid = labels.reshape(top, rows).T
    grid = grid[jax.random.permutation(jax.random.fold_in(own, 1), rows)]
    offset_by = jax.random.randint(jax.random.fold_in(own, 2), (rows, 1), 0, top)
    return jnp.take_along_axis(grid, (jnp.arange(top)[None, :] + offset_by) % top, axis=1)


def portions_of(count, total, reach, skew, full):
    portions = [(1 << 20) // math.isqrt(grade ** skew) + 1 for grade in range(1, count + 1)]
    largest = reach if full else min(reach, max(-(-total // count), total * portions[0] // sum(portions)))
    least = 1 if total - largest >= count - 1 else 0
    holding, surplus = [largest] + [least] * (count - 1), total - largest - least * (count - 1)
    while surplus > 0:
        movable = [i for i in range(1, count) if holding[i] < largest] or [i for i in range(1, count) if holding[i] < reach]
        pool, left = sum([portions[i] for i in movable]), surplus
        for i in movable:
            more = min(reach - holding[i], max(1, left * portions[i] // pool), surplus)
            holding[i] = holding[i] + more
            surplus = surplus - more
    return np.array(holding)


def bell_draw(own_key, dims, deviation, bound, shards=(), kind=jnp.bfloat16):
    gain = block_scale(own_key, dims, shards, -0.22, 0.18) if shards else 1.0
    array = jax.random.normal(own_key, dims, jnp.float32) * deviation * gain
    return jnp.minimum(jnp.maximum(array, -bound), bound).astype(kind)


def setup_inputs(seed: int = 0) -> dict:
    key_of = jax.random.split(jax.random.key(seed), 9)
    tokens = bell_draw(key_of[0], (TOKENS, D), 1.0, 6.0, ((0, 16),))
    cotangent = bell_draw(key_of[1], (TOKENS, D), 1.0, 6.0, ((0, 16),))
    group_prob = jnp.clip(0.25 + 0.75 * jax.random.uniform(key_of[2], (TOKENS,), jnp.float32) ** block_scale(key_of[2], (TOKENS,), ((0, 16),), -0.2, 0.2), 0.25, 1.0)
    expert_prob = jnp.clip(0.1 + 0.9 * jax.random.uniform(key_of[3], (TOKENS, TOP_K), jnp.float32) ** block_scale(key_of[3], (TOKENS, TOP_K), ((0, 16),), -0.2, 0.2), 0.1, 1.0)
    routing_keys = jax.random.split(jax.random.fold_in(key_of[4], 1), TOKENS // TOK_DEV)
    routing_turns = jax.random.permutation(jax.random.fold_in(key_of[4], 3), TOKENS // TOK_DEV)
    routing = jax.vmap(lambda own, number: assign_block(jax.random.fold_in(key_of[4], 2), own, number, TOK_DEV, EXPERTS, TOP_K, CAP, 2))(routing_keys, routing_turns).reshape((TOKENS, TOP_K))
    gate_weight = bell_draw(key_of[5], (EXPERTS, D, FF), D ** -0.5, 0.125, ((0, 16), (2, 32)))
    up_weight = bell_draw(key_of[6], (EXPERTS, D, FF), D ** -0.5, 0.125, ((0, 16), (2, 32)))
    down_weight = draw_down_weight(jax.random.fold_in(key_of[8], 71), 0)
    return {"tokens": tokens, "cotangent": cotangent, "group_prob": group_prob, "expert_prob": expert_prob, "routing": routing, "gate_weight": gate_weight, "up_weight": up_weight, "down_weight": down_weight}


def slot_targets(route_block):
    flat = route_block.reshape(-1).astype(jnp.int32)
    names = jnp.arange(EXPERTS, dtype=jnp.int32)
    onehot = (flat[:, None] == names[None, :]).astype(jnp.int32)
    before = (jnp.cumsum(onehot, axis=0) - onehot).astype(jnp.int32)
    place = jnp.sum(before * onehot, axis=1).astype(jnp.int32)
    return (flat * CAP + place).astype(jnp.int32)


def expert_pass(operands):
    rows_in, rows_scaled, w_gate, w_up, w_down = operands
    pre_gate = jnp.dot(rows_in, w_gate, preferred_element_type=jnp.float32)
    pre_up = jnp.dot(rows_in, w_up, preferred_element_type=jnp.float32)
    sigma = jax.nn.sigmoid(pre_gate)
    activated = pre_gate * sigma
    derivative = sigma * (1.0 + pre_gate * (1.0 - sigma))
    hidden = (activated * pre_up).astype(jnp.bfloat16)
    hidden_grad = jnp.dot(rows_scaled, w_down.T, preferred_element_type=jnp.float32)
    score = jnp.sum(hidden.astype(jnp.float32) * hidden_grad, axis=1)
    gate_pre = (hidden_grad * pre_up * derivative).astype(jnp.bfloat16)
    up_pre = (hidden_grad * activated).astype(jnp.bfloat16)
    down_sum = jnp.dot(hidden.T, rows_scaled, preferred_element_type=jnp.float32)
    gate_sum = jnp.dot(rows_in.T, gate_pre, preferred_element_type=jnp.float32)
    up_sum = jnp.dot(rows_in.T, up_pre, preferred_element_type=jnp.float32)
    slot_grad = jnp.dot(gate_pre, w_gate.T, preferred_element_type=jnp.float32)
    slot_grad = (slot_grad + jnp.dot(up_pre, w_up.T, preferred_element_type=jnp.float32)).astype(jnp.bfloat16)
    gate_norm = jnp.sum(gate_sum * gate_sum, axis=1) / FF
    up_norm = jnp.sum(up_sum * up_sum, axis=1) / FF
    down_norm = jnp.sum(down_sum * down_sum, axis=1) / D
    return (slot_grad, score, gate_sum.astype(jnp.bfloat16), up_sum.astype(jnp.bfloat16),
            down_sum.astype(jnp.bfloat16), gate_norm, up_norm, down_norm)


def to_experts(buffer):
    tail = buffer.shape[2:]
    shaped = buffer.reshape((N_EP, EXPERTS, CAP) + tail)
    shaped = jnp.swapaxes(shaped, 0, 1)
    return shaped.reshape((EXPERTS, N_EP * CAP) + tail)


def to_blocks(buffer):
    tail = buffer.shape[2:]
    shaped = buffer.reshape((EXPERTS, N_EP, CAP) + tail)
    shaped = jnp.swapaxes(shaped, 0, 1)
    return shaped.reshape((N_EP, EXPERTS * CAP) + tail)


def reference(tokens, cotangent, group_prob, expert_prob, routing, gate_weight, up_weight, down_weight):
    slot_count = TOK_DEV * TOP_K
    blocks = routing.reshape(N_EP, TOK_DEV, TOP_K)
    target = jax.vmap(slot_targets)(blocks)
    source = jnp.broadcast_to(jnp.arange(N_EP, dtype=jnp.int32)[:, None], target.shape)
    weight = group_prob[:, None] * expert_prob
    scaled = (weight[:, :, None] * cotangent.astype(jnp.float32)[:, None, :]).astype(jnp.bfloat16)
    token_slots = jnp.broadcast_to(tokens.reshape(N_EP, TOK_DEV, 1, D), (N_EP, TOK_DEV, TOP_K, D))
    token_slots = token_slots.reshape(N_EP, slot_count, D)
    scaled_slots = scaled.reshape(N_EP, slot_count, D)
    rows_in = jnp.zeros((N_EP, EXPERTS * CAP, D), jnp.bfloat16).at[source, target].set(token_slots)
    rows_scaled = jnp.zeros((N_EP, EXPERTS * CAP, D), jnp.bfloat16).at[source, target].set(scaled_slots)
    results = lax.map(expert_pass, (to_experts(rows_in), to_experts(rows_scaled), gate_weight, up_weight, down_weight))
    slot_grad, score, gate_grad, up_grad, down_grad, gate_norm, up_norm, down_norm = results
    returned = to_blocks(slot_grad)
    per_slot = jnp.take_along_axis(returned, target[:, :, None], axis=1)
    per_slot = per_slot.astype(jnp.float32).reshape(N_EP * TOK_DEV, TOP_K, D)
    token_grad = jnp.sum(per_slot, axis=1).astype(jnp.bfloat16)
    score_back = jnp.take_along_axis(to_blocks(score), target, axis=1).reshape(N_EP * TOK_DEV, TOP_K)
    slot_score = score_back / weight
    expert_prob_grad = group_prob[:, None] * slot_score
    group_prob_grad = jnp.sum(expert_prob * slot_score, axis=1)
    return (token_grad, group_prob_grad, expert_prob_grad, gate_grad, up_grad, down_grad,
            gate_norm, up_norm, down_norm)
```

```python
import functools
import jax
import jax.numpy as jnp
from jax import lax
from jax.experimental import pallas as pl
from jax.experimental.pallas import tpu as pltpu
from jax.sharding import PartitionSpec as P

MESH = pl.DeviceIdType.MESH
LANES = 128
F32 = jnp.float32
BF16 = jnp.bfloat16
CONTRACT_LAST = (((1,), (1,)), ((), ()))


def plane_peer(e, j, n_ep):
    if n_ep == 16:
        y, x = e // 4, e % 4
        return ((y + j // 4) % 4) * 4 + (x + j % 4) % 4
    return (e + j) % n_ep


def plane_source(e, j, n_ep):
    if n_ep == 16:
        y, x = e // 4, e % 4
        return ((y + 4 - j // 4) % 4) * 4 + (x + 4 - j % 4) % 4
    return (e + n_ep - j) % n_ep


def slot_rows(r, n_ep, cap):
    tok = r.shape[1]
    names = lax.broadcasted_iota(jnp.int32, (n_ep, tok), 0)
    first = (names == r[0:1, :]).astype(F32)
    second = (names == r[1:2, :]).astype(F32)
    earlier = lax.broadcasted_iota(jnp.int32, (tok, tok), 0) < lax.broadcasted_iota(
        jnp.int32, (tok, tok), 1
    )
    before = jnp.dot(
        (first + second).astype(BF16),
        jnp.where(earlier, 1.0, 0.0).astype(BF16),
        preferred_element_type=F32,
    )
    out = []
    for k, hot in enumerate((first, second)):
        place = jnp.sum(hot * before, axis=0, keepdims=True)
        out.append(r[k : k + 1, :].astype(F32) * float(cap) + place)
    return out


def body(
    n_ep, n_z, cap,
    r_ref, gp_ref, ep_ref, tok_hbm, cot_hbm, wg_hbm, wu_hbm, wd_hbm,
    tg_out, gg_out, ug_out, dg_out, gn_out, un_out, dn_out, epg_out, gpg_out,
    x, send, rows, wgu, wd, pre, hg, gpu, gput, hidt, prod,
    own, sib_send, sib_recv, dn_send, dn_recv, up_send, up_recv,
    sc_send, sc_recv, sm, sm_recv, sm_tot, sm_sib, sm_fin,
    fin, gat, tg, gg, ug, dg, dnacc,
    ld_sem, wl_sem, loc_sem, in_s, in_r, za_s, za_r, zb_s, zb_r, dx_s, dx_r, dy_s, dy_r,
    sc_s, sc_r, pt_s, pt_r, rd_s, rd_r, ru_s, ru_r, ms_s, ms_r, mx_s, mx_r, mg_s, mg_r,
    fa_s, fa_r, au_s, au_r, ad_s, ad_r, as_s, as_r, out_sem,
):
    e, tp = lax.axis_index("ep"), lax.axis_index("tp")
    z, c = tp // 2, tp % 2
    par = z % 2
    mine, other = par * 2, 2 - par * 2
    near, far = z + 1 - 2 * par, (z + n_z - 1 + 2 * par) % n_z
    up_z, dn_z = (z + 1) % n_z, (z + n_z - 1) % n_z
    tok, quarter = x.shape[0], rows.shape[3]
    slots = n_ep * cap
    half = slots // 2
    nd, nu = n_z // 2, n_z // 2 - 1
    qc = quarter // LANES
    sibling = (e, z * 2 + 1 - c)

    def at_z(other_z):
        return (e, other_z * 2 + c)

    def remote(src, dst, s_sem, r_sem, dev):
        return pltpu.make_async_remote_copy(
            src_ref=src, dst_ref=dst, send_sem=s_sem, recv_sem=r_sem,
            device_id=dev, device_id_type=MESH,
        )

    barrier = pltpu.get_barrier_semaphore()

    @pl.loop(1, n_ep)
    def _(j):
        pl.semaphore_signal(
            barrier, inc=1, device_id=(plane_peer(e, j, n_ep), tp), device_id_type=MESH
        )

    @pl.loop(1, n_z)
    def _(j):
        pl.semaphore_signal(barrier, inc=1, device_id=at_z((z + j) % n_z), device_id_type=MESH)

    pl.semaphore_signal(barrier, inc=1, device_id=sibling, device_id_type=MESH)

    start_col = pl.multiple_of(par * (2 * quarter), LANES)

    @pl.when(c == 0)
    def _():
        pltpu.make_async_copy(tok_hbm.at[:, pl.ds(start_col, 2 * quarter)], x, ld_sem).start()

    @pl.when(c == 1)
    def _():
        pltpu.make_async_copy(cot_hbm.at[:, pl.ds(start_col, 2 * quarter)], x, ld_sem).start()

    def weight_loads():
        out = []
        for q in range(4):
            span = pl.ds(q * quarter, quarter)
            out.append((wg_hbm.at[0, span, :], wgu.at[q, :, pl.ds(0, LANES)], wl_sem.at[q, 0]))
            out.append((wu_hbm.at[0, span, :], wgu.at[q, :, pl.ds(LANES, LANES)], wl_sem.at[q, 1]))
            out.append((wd_hbm.at[0, :, span], wd.at[q], wl_sem.at[q, 2]))
        return [pltpu.make_async_copy(*args) for args in out]

    for copy in weight_loads():
        copy.start()

    r = r_ref[...]
    weight = gp_ref[...] * ep_ref[...]
    w_eff = jnp.where(c == 0, jnp.ones_like(weight), weight)
    slot0, slot1 = slot_rows(r, n_ep, cap)
    pltpu.make_async_copy(tok_hbm.at[:, pl.ds(start_col, 2 * quarter)], x, ld_sem).wait()

    @pl.loop(0, slots // LANES)
    def _(i):
        at = pl.multiple_of(i * LANES, LANES)
        here = (lax.broadcasted_iota(jnp.int32, (LANES, tok), 0) + at).astype(F32)
        m0, m1 = here == slot0, here == slot1
        pick = jnp.where(m0 | m1, 1.0, 0.0).astype(BF16)
        scale = jnp.sum(
            jnp.where(m0, w_eff[0:1, :], 0.0) + jnp.where(m1, w_eff[1:2, :], 0.0),
            axis=1, keepdims=True,
        )
        got = scale * jnp.dot(pick, x[...], preferred_element_type=F32)
        send[0, pl.ds(at, LANES), :] = got[:, :quarter].astype(BF16)
        send[1, pl.ds(at, LANES), :] = got[:, quarter:].astype(BF16)

    pl.semaphore_wait(barrier, n_ep - 1 + n_z - 1 + 1)

    def block(b):
        return pl.ds(pl.multiple_of(b * cap, 16), cap)

    def own_block():
        return pltpu.make_async_copy(
            send.at[:, block(e), :], rows.at[c, pl.ds(mine, 2), block(e), :], loc_sem.at[0]
        )

    def in_copy(src_block, to, sender):
        return remote(
            send.at[:, block(src_block), :], rows.at[c, pl.ds(mine, 2), block(sender), :],
            in_s.at[src_block], in_r.at[sender], (to, tp),
        )

    def za_copy(s, first):
        ref = rows.at[c, first, block(s), :]
        return remote(ref, ref, za_s.at[s], za_r.at[s], at_z(near))

    def zb_copy(s, first):
        ref = rows.at[c, first + 1, block(s), :]
        return remote(ref, ref, zb_s.at[s], zb_r.at[s], at_z(far))

    def dx_copy(s, arr):
        ref = rows.at[arr, pl.ds(mine, 2), block(s), :]
        return remote(ref, ref, dx_s.at[s], dx_r.at[s], sibling)

    def dy_copy(s, arr):
        ref = rows.at[arr, pl.ds(other, 2), block(s), :]
        return remote(ref, ref, dy_s.at[s], dy_r.at[s], sibling)

    own_block().start()

    @pl.loop(1, n_ep)
    def _(j):
        p = plane_peer(e, j, n_ep)
        in_copy(p, p, e).start()

    own_block().wait()
    za_copy(e, mine).start()
    zb_copy(e, mine).start()
    dx_copy(e, c).start()

    @pl.loop(1, n_ep)
    def _(j):
        s = plane_source(e, j, n_ep)
        in_copy(s, s, s).wait_recv()
        za_copy(s, mine).start()
        zb_copy(s, mine).start()
        dx_copy(s, c).start()

    @pl.loop(0, n_ep)
    def _(j):
        s = plane_source(e, j, n_ep)
        za_copy(s, other).wait_recv()
        zb_copy(s, other).wait_recv()
        dy_copy(s, c).start()

    for copy in weight_loads():
        copy.wait()

    @pl.loop(0, n_ep)
    def _(j):
        s = plane_source(e, j, n_ep)
        dx_copy(s, 1 - c).wait_recv()
        dy_copy(s, 1 - c).wait_recv()

    pre[...] = jnp.zeros_like(pre)
    hg[...] = jnp.zeros_like(hg)

    @pl.loop(0, 4)
    def _(q):
        pre[...] += jnp.dot(rows[0, q], wgu[q], preferred_element_type=F32)
        hg[...] += lax.dot_general(rows[1, q], wd[q], CONTRACT_LAST, preferred_element_type=F32)

    @pl.loop(0, slots // LANES)
    def _(i):
        at = pl.ds(pl.multiple_of(i * LANES, LANES), LANES)
        gate, upv, grad = pre[at, :LANES], pre[at, LANES:], hg[at, :]
        sigma = jax.nn.sigmoid(gate)
        activated = gate * sigma
        derivative = sigma * (1.0 + gate * (1.0 - sigma))
        hidden = (activated * upv).astype(BF16).astype(F32)
        gate_pre = (grad * upv * derivative).astype(BF16).astype(F32)
        up_pre = (grad * activated).astype(BF16).astype(F32)
        prod[at, :] = hidden * grad
        gpu[at, :LANES] = gate_pre.astype(BF16)
        gpu[at, LANES:] = up_pre.astype(BF16)
        gput[:LANES, at] = gate_pre.T.astype(BF16)
        gput[LANES:, at] = up_pre.T.astype(BF16)
        hidt[:, at] = hidden.T.astype(BF16)

    ones = jnp.ones((8, LANES), F32)
    for b in range(n_ep):
        row = lax.dot_general(
            ones, prod[b * cap : (b + 1) * cap, :], CONTRACT_LAST,
            precision=lax.Precision.HIGHEST, preferred_element_type=F32,
        )
        sc_send[b, :, :cap] = row[0:1, :]

    def sc_copy(to, sender):
        return remote(sc_send.at[to], sc_recv.at[sender], sc_s.at[to], sc_r.at[sender], (to, tp))

    @pl.loop(1, n_ep)
    def _(j):
        p = plane_peer(e, j, n_ep)
        sc_copy(p, e).start()

    keep = pl.ds(pl.multiple_of(c * half, 16), half)
    give = pl.ds(pl.multiple_of((1 - c) * half, 16), half)

    def pt_copy(o):
        return remote(sib_send.at[o], sib_recv.at[o], pt_s.at[o], pt_r.at[o], sibling)

    @pl.loop(0, 4)
    def _(q):
        given = lax.dot_general(gpu[give, :], wgu[q], CONTRACT_LAST, preferred_element_type=F32)
        for i in range(qc):
            sib_send[q * qc + i] = given[:, i * LANES : (i + 1) * LANES].astype(BF16)
        for i in range(qc):
            pt_copy(q * qc + i).start()
        kept = lax.dot_general(gpu[keep, :], wgu[q], CONTRACT_LAST, preferred_element_type=F32)
        for i in range(qc):
            own[q * qc + i] = kept[:, i * LANES : (i + 1) * LANES]

    dnacc[...] = jnp.zeros_like(dnacc)

    def weight_quarter(q):
        down = jnp.dot(hidt[...], rows[1, q], preferred_element_type=F32)
        dg[:, q * quarter : (q + 1) * quarter] = down.astype(BF16)
        square = down * down
        dnacc[...] += sum(square[:, i * LANES : (i + 1) * LANES] for i in range(qc))
        for k, target in enumerate((gg, ug)):
            both = jnp.dot(
                gput[k * LANES : (k + 1) * LANES, :], rows[0, q], preferred_element_type=F32
            )
            norm = jnp.sum(both * both, axis=0, keepdims=True)
            for i in range(qc):
                sm[q * qc + i, :, k * LANES : (k + 1) * LANES] = norm[:, i * LANES : (i + 1) * LANES]
            target[q * quarter : (q + 1) * quarter, :] = both.T.astype(BF16)

    def grad_stores():
        return [
            pltpu.make_async_copy(gg, gg_out.at[0], out_sem.at[0]),
            pltpu.make_async_copy(ug, ug_out.at[0], out_sem.at[1]),
            pltpu.make_async_copy(dg, dg_out.at[0], out_sem.at[2]),
        ]

    def own_scores():
        sc_recv[e] = sc_send[e]

    def ms_copy(o, sender):
        return remote(sm.at[o], sm_recv.at[sender], ms_s.at[o], ms_r.at[sender], at_z(o))

    def mx_copy():
        return remote(sm_tot, sm_sib, mx_s.at[0], mx_r.at[0], sibling)

    def mg_copy(piece, to):
        return remote(sm_fin.at[piece], sm_fin.at[piece], mg_s.at[to], mg_r.at[piece], at_z(to))

    score_rows = tok // LANES

    def small_start():
        own_scores()

        @pl.loop(1, n_ep)
        def _(j):
            s = plane_source(e, j, n_ep)
            sc_copy(s, s).wait_recv()

        got = sc_recv[...].reshape(n_ep, sc_recv.shape[2])
        fill = jnp.zeros((LANES - n_ep, got.shape[1]), F32)
        columns = jnp.concatenate([got, fill], axis=0).T
        totals = [jnp.zeros((1, tok), F32), jnp.zeros((1, tok), F32)]
        lane = lax.broadcasted_iota(jnp.int32, (cap, tok), 0)
        for s in range(n_ep):
            here = (lane + s * cap).astype(F32)
            column = columns[:cap, s : s + 1]
            for k, slot in enumerate((slot0, slot1)):
                totals[k] += jnp.sum(jnp.where(here == slot, column, 0.0), axis=0, keepdims=True)
        sm[:, :, 2 * LANES :] = jnp.zeros((n_z, 1, LANES), F32)
        for k in range(2):
            for h in range(score_rows):
                sm[k * score_rows + h, :, 2 * LANES :] = totals[k][:, h * LANES : (h + 1) * LANES]

        @pl.loop(1, n_z)
        def _(j):
            o = (z + j) % n_z
            ms_copy(o, z).start()

    def small_middle():
        @pl.loop(1, n_z)
        def _(j):
            s = (z + j) % n_z
            ms_copy(s, s).wait_recv()

        sm_recv[z] = sm[z]
        sm_tot[...] = jnp.sum(sm_recv[...], axis=0)
        mx_copy().start()

    def small_end():
        mx_copy().wait_recv()
        sm_fin[z] = sm_tot[...] + sm_sib[...]

        @pl.loop(1, n_z)
        def _(j):
            mg_copy(z, (z + j) % n_z).start()

    sub = half // 2

    def part(h):
        return pl.ds(h * sub, sub)

    def rd_copy(t, h):
        return remote(
            dn_send.at[t, part(h), :], dn_recv.at[t, part(h), :],
            rd_s.at[t, h], rd_r.at[t, h], at_z(dn_z),
        )

    def ru_copy(t, h):
        return remote(
            up_send.at[t, part(h), :], up_recv.at[t, part(h), :],
            ru_s.at[t, h], ru_r.at[t, h], at_z(up_z),
        )

    def chip_sum(o, h):
        return own[o, part(h), :] + sib_recv[o, part(h), :].astype(F32)

    for t in range(nd):
        o_dn, o_up = (z + n_z - nd + t) % n_z, (z + nu - t + n_z) % n_z
        pt_copy(o_dn).wait_recv()
        pt_copy(o_up).wait_recv()
        for h in range(2):
            total = chip_sum(o_dn, h)
            if t > 0:
                rd_copy(t - 1, h).wait_recv()
                total += dn_recv[t - 1, part(h), :].astype(F32)
            dn_send[t, part(h), :] = total.astype(BF16)
            rd_copy(t, h).start()
            if t < nu:
                total = chip_sum(o_up, h)
                if t > 0:
                    ru_copy(t - 1, h).wait_recv()
                    total += up_recv[t - 1, part(h), :].astype(F32)
                up_send[t, part(h), :] = total.astype(BF16)
                ru_copy(t, h).start()
        if n_z == 16:
            if t < 4:
                weight_quarter(t)
            if t == 3:
                small_start()
                for copy in grad_stores():
                    copy.start()
            if t == 6:
                small_middle()
        elif t == 0:
            for q in range(4):
                weight_quarter(q)
            small_start()
            for copy in grad_stores():
                copy.start()
            small_middle()

    for h in range(2):
        total = chip_sum(z, h)
        ru_copy(nu - 1, h).wait_recv()
        total += up_recv[nu - 1, part(h), :].astype(F32)
        rd_copy(nd - 1, h).wait_recv()
        total += dn_recv[nd - 1, part(h), :].astype(F32)
        fin[part(h), :] = total.astype(BF16)

    per_core = n_ep // 2
    ce = e // per_core

    def fa_copy(i, to, sender):
        return remote(
            fin.at[pl.ds(i * cap, cap), :], gat.at[block(sender), :],
            fa_s.at[i], fa_r.at[sender], (to, tp),
        )

    def fa_local(i):
        return pltpu.make_async_copy(
            fin.at[pl.ds(i * cap, cap), :], gat.at[block(e), :], loc_sem.at[1]
        )

    for i in range(per_core):
        b = c * per_core + i

        @pl.when(b != e)
        def _():
            fa_copy(i, b, e).start()

        @pl.when(b == e)
        def _():
            fa_local(i).start()

    small_end()

    def chunk(o):
        return tg.at[:, pl.ds(pl.multiple_of(o * LANES, LANES), LANES)]

    def au_copy(t, o):
        return remote(chunk(o), chunk(o), au_s.at[t], au_r.at[t], at_z(up_z))

    def ad_copy(t, o):
        return remote(chunk(o), chunk(o), ad_s.at[t], ad_r.at[t], at_z(dn_z))

    def as_copy(o):
        return remote(chunk(o), chunk(o), as_s.at[o], as_r.at[o], sibling)

    @pl.when(c == ce)
    def _():
        fa_local(0).wait()

        @pl.loop(1, n_ep)
        def _(j):
            s = (e + j) % n_ep
            fa_copy(0, s, s).wait_recv()

        acc = jnp.zeros((tok, LANES), F32)
        lane = lax.broadcasted_iota(jnp.int32, (slots, tok), 0).astype(F32)
        pick = jnp.where((lane == slot0) | (lane == slot1), 1.0, 0.0)
        acc = jnp.dot(pick.T.astype(BF16), gat[...], preferred_element_type=F32)
        tg[:, pl.ds(pl.multiple_of(z * LANES, LANES), LANES)] = acc.astype(BF16)
        au_copy(1, z).start()
        ad_copy(1, z).start()
        as_copy(z).start()
        for t in range(1, nd + 1):
            if t <= nu:
                o = (z + n_z - t) % n_z
                au_copy(t, o).wait_recv()
                if t < nu:
                    au_copy(t + 1, o).start()
                as_copy(o).start()
            o = (z + t) % n_z
            ad_copy(t, o).wait_recv()
            if t < nd:
                ad_copy(t + 1, o).start()
            as_copy(o).start()

    @pl.loop(1, n_z)
    def _(j):
        o = (z + j) % n_z
        mg_copy(o, o).wait_recv()

    units = float(LANES * 2 * n_z)
    for o in range(n_z):
        gn_out[:, o * LANES : (o + 1) * LANES] = sm_fin[o, :, :LANES] / units
        un_out[:, o * LANES : (o + 1) * LANES] = sm_fin[o, :, LANES : 2 * LANES] / units
    dn_out[...] = lax.dot_general(
        jnp.ones((8, LANES), F32), dnacc[...], CONTRACT_LAST,
        precision=lax.Precision.HIGHEST, preferred_element_type=F32,
    )[0:1, :] / float(LANES * n_z)
    for h in range(score_rows):
        at = slice(h * LANES, (h + 1) * LANES)
        gp = gp_ref[:, at]
        total = jnp.zeros((1, LANES), F32)
        for k in range(2):
            ep = ep_ref[k : k + 1, at]
            score = sm_fin[k * score_rows + h, :, 2 * LANES :] / (gp * ep)
            epg_out[k : k + 1, at] = gp * score
            total += ep * score
        gpg_out[:, at] = total

    @pl.when(c != ce)
    def _():
        @pl.loop(0, n_z)
        def _(o):
            as_copy(o).wait_recv()

    tg_store = pltpu.make_async_copy(tg, tg_out, out_sem.at[3])
    tg_store.start()

    for copy in grad_stores():
        copy.wait()

    @pl.loop(1, n_ep)
    def _(j):
        p = plane_peer(e, j, n_ep)
        in_copy(p, p, e).wait_send()
        sc_copy(p, e).wait_send()

    @pl.loop(0, n_ep)
    def _(s):
        za_copy(s, mine).wait_send()
        zb_copy(s, mine).wait_send()
        dx_copy(s, c).wait_send()
        dy_copy(s, c).wait_send()

    @pl.loop(0, n_z)
    def _(o):
        pt_copy(o).wait_send()

    @pl.loop(1, n_z)
    def _(j):
        o = (z + j) % n_z
        ms_copy(o, z).wait_send()
        mg_copy(z, o).wait_send()

    mx_copy().wait_send()
    for h in range(2):
        for t in range(nd):
            rd_copy(t, h).wait_send()
        for t in range(nu):
            ru_copy(t, h).wait_send()

    for i in range(per_core):
        b = c * per_core + i

        @pl.when(b != e)
        def _():
            fa_copy(i, b, e).wait_send()

    @pl.when(c == ce)
    def _():
        for t in range(1, nu + 1):
            au_copy(t, z).wait_send()
        for t in range(1, nd + 1):
            ad_copy(t, z).wait_send()

        @pl.loop(0, n_z)
        def _(o):
            as_copy(o).wait_send()

    tg_store.wait()


def local(tokens, cotangent, group_prob, expert_prob, routing, gate_weight, up_weight, down_weight):
    tok, width = tokens.shape
    n_ep = lax.axis_size("ep")
    n_z = lax.axis_size("tp") // 2
    cap = 3 * tok * 2 // (2 * n_ep)
    slots = n_ep * cap
    half = slots // 2
    quarter = width // 4
    unit = gate_weight.shape[2]
    nd, nu = n_z // 2, n_z // 2 - 1
    scw = -(-cap // LANES) * LANES
    dma = pltpu.SemaphoreType.DMA
    vm = pltpu.VMEM
    any_spec = pl.BlockSpec(memory_space=pl.ANY)
    vm_spec = pl.BlockSpec(memory_space=pltpu.VMEM)
    outs = pl.pallas_call(
        functools.partial(body, n_ep, n_z, cap),
        out_shape=(
            jax.ShapeDtypeStruct((tok, width), BF16),
            jax.ShapeDtypeStruct((1, width, unit), BF16),
            jax.ShapeDtypeStruct((1, width, unit), BF16),
            jax.ShapeDtypeStruct((1, unit, width), BF16),
            jax.ShapeDtypeStruct((1, width), F32),
            jax.ShapeDtypeStruct((1, width), F32),
            jax.ShapeDtypeStruct((1, unit), F32),
            jax.ShapeDtypeStruct((2, tok), F32),
            jax.ShapeDtypeStruct((1, tok), F32),
        ),
        in_specs=[vm_spec] * 3 + [any_spec] * 5,
        out_specs=(any_spec,) * 4 + (vm_spec,) * 5,
        scratch_shapes=[
            vm((tok, 2 * quarter), BF16),
            vm((2, slots, quarter), BF16),
            vm((2, 4, slots, quarter), BF16),
            vm((4, quarter, 2 * unit), BF16),
            vm((4, unit, quarter), BF16),
            vm((slots, 2 * unit), F32),
            vm((slots, unit), F32),
            vm((slots, 2 * unit), BF16),
            vm((2 * unit, slots), BF16),
            vm((unit, slots), BF16),
            vm((slots, unit), F32),
            vm((n_z, half, LANES), F32),
            vm((n_z, half, LANES), BF16),
            vm((n_z, half, LANES), BF16),
            vm((nd, half, LANES), BF16),
            vm((nd, half, LANES), BF16),
            vm((nu, half, LANES), BF16),
            vm((nu, half, LANES), BF16),
            vm((n_ep, 1, scw), F32),
            vm((n_ep, 1, scw), F32),
            vm((n_z, 1, 3 * LANES), F32),
            vm((n_z, 1, 3 * LANES), F32),
            vm((1, 3 * LANES), F32),
            vm((1, 3 * LANES), F32),
            vm((n_z, 1, 3 * LANES), F32),
            vm((half, LANES), BF16),
            vm((slots, LANES), BF16),
            vm((tok, width), BF16),
            vm((width, unit), BF16),
            vm((width, unit), BF16),
            vm((unit, width), BF16),
            vm((unit, LANES), F32),
            dma, dma((4, 3)), dma((2,)),
            dma((n_ep,)), dma((n_ep,)), dma((n_ep,)), dma((n_ep,)), dma((n_ep,)), dma((n_ep,)),
            dma((n_ep,)), dma((n_ep,)), dma((n_ep,)), dma((n_ep,)),
            dma((n_ep,)), dma((n_ep,)),
            dma((n_z,)), dma((n_z,)),
            dma((nd, 2)), dma((nd, 2)), dma((nu, 2)), dma((nu, 2)),
            dma((n_z,)), dma((n_z,)), dma((1,)), dma((1,)), dma((n_z,)), dma((n_z,)),
            dma((n_ep // 2,)), dma((n_ep,)),
            dma((nu + 1,)), dma((nu + 1,)), dma((nd + 1,)), dma((nd + 1,)),
            dma((n_z,)), dma((n_z,)),
            dma((4,)),
        ],
        compiler_params=pltpu.CompilerParams(
            collective_id=0, has_side_effects=True, vmem_limit_bytes=56 * 1024 * 1024
        ),
    )(
        routing.T, group_prob[None, :], expert_prob.T, tokens, cotangent,
        gate_weight, up_weight, down_weight,
    )
    tg, gg, ug, dg, gn, un, dn, epg, gpg = outs
    return tg, gpg[0], epg.T, gg, ug, dg, gn, un, dn


def solution(mesh):
    return jax.shard_map(
        local,
        mesh=mesh,
        in_specs=(
            P("ep", None),
            P("ep", None),
            P("ep"),
            P("ep", None),
            P("ep", None),
            P("ep", None, "tp"),
            P("ep", None, "tp"),
            P("ep", "tp", None),
        ),
        out_specs=(
            P("ep", None),
            P("ep"),
            P("ep", None),
            P("ep", None, "tp"),
            P("ep", None, "tp"),
            P("ep", "tp", None),
            P("ep", None),
            P("ep", None),
            P("ep", "tp"),
        ),
        check_vma=False,
    )
```

```python
import functools
import jax
import jax.numpy as jnp
from jax import lax
from jax.experimental import pallas as pl
from jax.experimental.pallas import tpu as pltpu
from jax.sharding import PartitionSpec as P

MESH = pl.DeviceIdType.MESH
LANES = 128
F32 = jnp.float32
BF16 = jnp.bfloat16
CONTRACT_LAST = (((1,), (1,)), ((), ()))
SUM_PIECES = 4
GATHER_PIECES = 2
GATHER_CORE = 1


def plane_peer(e, j, n_ep):
    if n_ep == 16:
        y, x = e // 4, e % 4
        return ((y + j // 4) % 4) * 4 + (x + j % 4) % 4
    return (e + j) % n_ep


def plane_source(e, j, n_ep):
    if n_ep == 16:
        y, x = e // 4, e % 4
        return ((y + 4 - j // 4) % 4) * 4 + (x + 4 - j % 4) % 4
    return (e + n_ep - j) % n_ep


def slot_rows(r, n_ep, cap):
    tok = r.shape[1]
    names = lax.broadcasted_iota(jnp.int32, (n_ep, tok), 0)
    first = (names == r[0:1, :]).astype(F32)
    second = (names == r[1:2, :]).astype(F32)
    earlier = lax.broadcasted_iota(jnp.int32, (tok, tok), 0) < lax.broadcasted_iota(
        jnp.int32, (tok, tok), 1
    )
    before = jnp.dot(
        (first + second).astype(BF16),
        jnp.where(earlier, 1.0, 0.0).astype(BF16),
        preferred_element_type=F32,
    )
    out = []
    for k, hot in enumerate((first, second)):
        place = jnp.sum(hot * before, axis=0, keepdims=True)
        out.append(r[k : k + 1, :].astype(F32) * float(cap) + place)
    return out


def body(
    n_ep, n_z, cap,
    r_ref, gp_ref, ep_ref, tok_hbm, cot_hbm, wg_hbm, wu_hbm, wd_hbm,
    tg_out, gg_out, ug_out, dg_out, gn_out, un_out, dn_out, epg_out, gpg_out,
    x, send, rows, wgu, wd, pre, hg, gpu, gput, hidt, prod,
    own, sib_send, sib_recv, dn_send, dn_recv, up_send, up_recv,
    sc_send, sc_recv, sm, sm_recv, sm_tot, sm_sib, sm_fin,
    fin, gat, tg, gg, ug, dg, dnacc,
    ld_sem, wl_sem, loc_sem, in_s, in_r, za_s, za_r, zb_s, zb_r, dx_s, dx_r, dy_s, dy_r,
    sc_s, sc_r, pt_s, pt_r, rd_s, rd_r, ru_s, ru_r, ms_s, ms_r, mx_s, mx_r, mg_s, mg_r,
    fa_s, fa_r, au_s, au_r, ad_s, ad_r, as_s, as_r, out_sem, met4, met8, pickt,
):
    e, tp = lax.axis_index("ep"), lax.axis_index("tp")
    z, c = tp // 2, tp % 2
    par = z % 2
    mine, other = par * 2, 2 - par * 2
    near, far = z + 1 - 2 * par, (z + n_z - 1 + 2 * par) % n_z
    up_z, dn_z = (z + 1) % n_z, (z + n_z - 1) % n_z
    tok, quarter = x.shape[0], rows.shape[3]
    slots = n_ep * cap
    half = slots // 2
    nd, nu = n_z // 2, n_z // 2 - 1
    qc = quarter // LANES
    sibling = (e, z * 2 + 1 - c)

    def at_z(other_z):
        return (e, other_z * 2 + c)

    def remote(src, dst, s_sem, r_sem, dev):
        return pltpu.make_async_remote_copy(
            src_ref=src, dst_ref=dst, send_sem=s_sem, recv_sem=r_sem,
            device_id=dev, device_id_type=MESH,
        )

    barrier = pltpu.get_barrier_semaphore()

    @pl.loop(1, n_ep)
    def _(j):
        pl.semaphore_signal(
            barrier, inc=1, device_id=(plane_peer(e, j, n_ep), tp), device_id_type=MESH
        )

    for step in (1, 2):
        for o in (z + step, z + n_z - step):
            pl.semaphore_signal(barrier, inc=1, device_id=at_z(o % n_z), device_id_type=MESH)
    pl.semaphore_signal(barrier, inc=1, device_id=sibling, device_id_type=MESH)

    def greet(sem, step):
        for o in (z + step, z + n_z - step):
            pl.semaphore_signal(sem, inc=1, device_id=at_z(o % n_z), device_id_type=MESH)

    start_col = pl.multiple_of(par * (2 * quarter), LANES)

    @pl.when(c == 0)
    def _():
        pltpu.make_async_copy(tok_hbm.at[:, pl.ds(start_col, 2 * quarter)], x, ld_sem).start()

    @pl.when(c == 1)
    def _():
        pltpu.make_async_copy(cot_hbm.at[:, pl.ds(start_col, 2 * quarter)], x, ld_sem).start()

    def weight_loads():
        out = []
        for q in range(4):
            span = pl.ds(q * quarter, quarter)
            out.append((wg_hbm.at[0, span, :], wgu.at[q, :, pl.ds(0, LANES)], wl_sem.at[q, 0]))
            out.append((wu_hbm.at[0, span, :], wgu.at[q, :, pl.ds(LANES, LANES)], wl_sem.at[q, 1]))
            out.append((wd_hbm.at[0, :, span], wd.at[q], wl_sem.at[q, 2]))
        return [pltpu.make_async_copy(*args) for args in out]

    for copy in weight_loads():
        copy.start()

    r = r_ref[...]
    weight = gp_ref[...] * ep_ref[...]
    w_eff = jnp.where(c == 0, jnp.ones_like(weight), weight)
    slot0, slot1 = slot_rows(r, n_ep, cap)
    pltpu.make_async_copy(tok_hbm.at[:, pl.ds(start_col, 2 * quarter)], x, ld_sem).wait()

    @pl.loop(0, slots // LANES)
    def _(i):
        at = pl.multiple_of(i * LANES, LANES)
        here = (lax.broadcasted_iota(jnp.int32, (LANES, tok), 0) + at).astype(F32)
        m0, m1 = here == slot0, here == slot1
        pick = jnp.where(m0 | m1, 1.0, 0.0).astype(BF16)
        scale = jnp.sum(
            jnp.where(m0, w_eff[0:1, :], 0.0) + jnp.where(m1, w_eff[1:2, :], 0.0),
            axis=1, keepdims=True,
        )
        got = scale * jnp.dot(pick, x[...], preferred_element_type=F32)
        send[0, pl.ds(at, LANES), :] = got[:, :quarter].astype(BF16)
        send[1, pl.ds(at, LANES), :] = got[:, quarter:].astype(BF16)

    pl.semaphore_wait(barrier, n_ep - 1 + 4 + 1)
    greet(met4, 2)

    def block(b):
        return pl.ds(pl.multiple_of(b * cap, 16), cap)

    def own_block():
        return pltpu.make_async_copy(
            send.at[:, block(e), :], rows.at[c, pl.ds(mine, 2), block(e), :], loc_sem.at[0]
        )

    def in_copy(src_block, to, sender):
        return remote(
            send.at[:, block(src_block), :], rows.at[c, pl.ds(mine, 2), block(sender), :],
            in_s.at[src_block], in_r.at[sender], (to, tp),
        )

    def za_copy(s, first):
        ref = rows.at[c, first, block(s), :]
        return remote(ref, ref, za_s.at[s], za_r.at[s], at_z(near))

    def zb_copy(s, first):
        ref = rows.at[c, first + 1, block(s), :]
        return remote(ref, ref, zb_s.at[s], zb_r.at[s], at_z(far))

    def dx_copy(s, arr):
        ref = rows.at[arr, pl.ds(mine, 2), block(s), :]
        return remote(ref, ref, dx_s.at[s], dx_r.at[s], sibling)

    def dy_copy(s, arr):
        ref = rows.at[arr, pl.ds(other, 2), block(s), :]
        return remote(ref, ref, dy_s.at[s], dy_r.at[s], sibling)

    own_block().start()

    @pl.loop(1, n_ep)
    def _(j):
        p = plane_peer(e, j, n_ep)
        in_copy(p, p, e).start()

    own_block().wait()
    za_copy(e, mine).start()
    zb_copy(e, mine).start()
    dx_copy(e, c).start()

    @pl.loop(1, n_ep)
    def _(j):
        s = plane_source(e, j, n_ep)
        in_copy(s, s, s).wait_recv()
        za_copy(s, mine).start()
        zb_copy(s, mine).start()
        dx_copy(s, c).start()

    pl.semaphore_wait(met4, 2)
    greet(met8, 4)

    @pl.loop(0, n_ep)
    def _(j):
        s = plane_source(e, j, n_ep)
        za_copy(s, other).wait_recv()
        zb_copy(s, other).wait_recv()
        dy_copy(s, c).start()

    for copy in weight_loads():
        copy.wait()

    @pl.loop(0, n_ep)
    def _(j):
        s = plane_source(e, j, n_ep)
        dx_copy(s, 1 - c).wait_recv()
        dy_copy(s, 1 - c).wait_recv()

    pl.semaphore_wait(met8, 2)

    pre[...] = jnp.zeros_like(pre)
    hg[...] = jnp.zeros_like(hg)

    @pl.loop(0, 4)
    def _(q):
        pre[...] += jnp.dot(rows[0, q], wgu[q], preferred_element_type=F32)
        hg[...] += lax.dot_general(rows[1, q], wd[q], CONTRACT_LAST, preferred_element_type=F32)

    @pl.loop(0, slots // LANES)
    def _(i):
        at = pl.ds(pl.multiple_of(i * LANES, LANES), LANES)
        gate, upv, grad = pre[at, :LANES], pre[at, LANES:], hg[at, :]
        sigma = jax.nn.sigmoid(gate)
        activated = gate * sigma
        derivative = sigma * (1.0 + gate * (1.0 - sigma))
        hidden = (activated * upv).astype(BF16).astype(F32)
        gate_pre = (grad * upv * derivative).astype(BF16).astype(F32)
        up_pre = (grad * activated).astype(BF16).astype(F32)
        prod[at, :] = hidden * grad
        gpu[at, :LANES] = gate_pre.astype(BF16)
        gpu[at, LANES:] = up_pre.astype(BF16)
        gput[:LANES, at] = gate_pre.T.astype(BF16)
        gput[LANES:, at] = up_pre.T.astype(BF16)
        hidt[:, at] = hidden.T.astype(BF16)

    ones = jnp.ones((8, LANES), F32)
    for b in range(n_ep):
        row = lax.dot_general(
            ones, prod[b * cap : (b + 1) * cap, :], CONTRACT_LAST,
            precision=lax.Precision.HIGHEST, preferred_element_type=F32,
        )
        sc_send[b, :, :cap] = row[0:1, :]

    def sc_copy(to, sender):
        return remote(sc_send.at[to], sc_recv.at[sender], sc_s.at[to], sc_r.at[sender], (to, tp))

    @pl.loop(1, n_ep)
    def _(j):
        p = plane_peer(e, j, n_ep)
        sc_copy(p, e).start()

    keep = pl.ds(pl.multiple_of(c * half, 16), half)
    give = pl.ds(pl.multiple_of((1 - c) * half, 16), half)

    def pt_copy(o):
        return remote(sib_send.at[o], sib_recv.at[o], pt_s.at[o], pt_r.at[o], sibling)

    @pl.loop(0, 4)
    def _(q):
        given = lax.dot_general(gpu[give, :], wgu[q], CONTRACT_LAST, preferred_element_type=F32)
        for i in range(qc):
            sib_send[q * qc + i] = given[:, i * LANES : (i + 1) * LANES].astype(BF16)
        for i in range(qc):
            pt_copy(q * qc + i).start()
        kept = lax.dot_general(gpu[keep, :], wgu[q], CONTRACT_LAST, preferred_element_type=F32)
        for i in range(qc):
            own[q * qc + i] = kept[:, i * LANES : (i + 1) * LANES]

    dnacc[...] = jnp.zeros_like(dnacc)

    def down_piece(q):
        down = jnp.dot(hidt[...], rows[1, q], preferred_element_type=F32)
        dg[:, q * quarter : (q + 1) * quarter] = down.astype(BF16)
        square = down * down
        dnacc[...] += sum(square[:, i * LANES : (i + 1) * LANES] for i in range(qc))

    def in_piece(k, q):
        target = (gg, ug)[k]
        both = jnp.dot(gput[k * LANES : (k + 1) * LANES, :], rows[0, q], preferred_element_type=F32)
        norm = jnp.sum(both * both, axis=0, keepdims=True)
        for i in range(qc):
            sm[q * qc + i, :, k * LANES : (k + 1) * LANES] = norm[:, i * LANES : (i + 1) * LANES]
        target[q * quarter : (q + 1) * quarter, :] = both.T.astype(BF16)

    def pick_piece():
        lane = lax.broadcasted_iota(jnp.int32, (slots, tok), 0).astype(F32)
        pick = jnp.where((lane == slot0) | (lane == slot1), 1.0, 0.0)
        pickt[...] = pick.T.astype(BF16)

    def grad_stores():
        return [
            pltpu.make_async_copy(gg, gg_out.at[0], out_sem.at[0]),
            pltpu.make_async_copy(ug, ug_out.at[0], out_sem.at[1]),
            pltpu.make_async_copy(dg, dg_out.at[0], out_sem.at[2]),
        ]

    def own_scores():
        sc_recv[e] = sc_send[e]

    def ms_copy(o, sender):
        return remote(sm.at[o], sm_recv.at[sender], ms_s.at[o], ms_r.at[sender], at_z(o))

    def mx_copy():
        return remote(sm_tot, sm_sib, mx_s.at[0], mx_r.at[0], sibling)

    def mg_copy(piece, to):
        return remote(sm_fin.at[piece], sm_fin.at[piece], mg_s.at[to], mg_r.at[piece], at_z(to))

    score_rows = tok // LANES

    def small_start():
        own_scores()

        @pl.loop(1, n_ep)
        def _(j):
            s = plane_source(e, j, n_ep)
            sc_copy(s, s).wait_recv()

        got = sc_recv[...].reshape(n_ep, sc_recv.shape[2])
        fill = jnp.zeros((LANES - n_ep, got.shape[1]), F32)
        columns = jnp.concatenate([got, fill], axis=0).T
        totals = [jnp.zeros((1, tok), F32), jnp.zeros((1, tok), F32)]
        lane = lax.broadcasted_iota(jnp.int32, (cap, tok), 0)
        for s in range(n_ep):
            here = (lane + s * cap).astype(F32)
            column = columns[:cap, s : s + 1]
            for k, slot in enumerate((slot0, slot1)):
                totals[k] += jnp.sum(jnp.where(here == slot, column, 0.0), axis=0, keepdims=True)
        sm[:, :, 2 * LANES :] = jnp.zeros((n_z, 1, LANES), F32)
        for k in range(2):
            for h in range(score_rows):
                sm[k * score_rows + h, :, 2 * LANES :] = totals[k][:, h * LANES : (h + 1) * LANES]

        @pl.loop(1, n_z)
        def _(j):
            o = (z + j) % n_z
            ms_copy(o, z).start()

    def small_middle():
        @pl.loop(1, n_z)
        def _(j):
            s = (z + j) % n_z
            ms_copy(s, s).wait_recv()

        sm_recv[z] = sm[z]
        sm_tot[...] = jnp.sum(sm_recv[...], axis=0)
        mx_copy().start()

    def small_end():
        mx_copy().wait_recv()
        sm_fin[z] = sm_tot[...] + sm_sib[...]

        @pl.loop(1, n_z)
        def _(j):
            mg_copy(z, (z + j) % n_z).start()

    def store_start():
        for copy in grad_stores():
            copy.start()

    work = []
    for q in range(4):
        work += [functools.partial(down_piece, q)]
        work += [functools.partial(in_piece, 0, q), functools.partial(in_piece, 1, q)]
    work += [small_start, store_start, pick_piece]

    sub = half // SUM_PIECES

    def part(h):
        return pl.ds(h * sub, sub)

    def rd_copy(t, h):
        return remote(
            dn_send.at[t, part(h), :], dn_recv.at[t, part(h), :],
            rd_s.at[t, h], rd_r.at[t, h], at_z(dn_z),
        )

    def ru_copy(t, h):
        return remote(
            up_send.at[t, part(h), :], up_recv.at[t, part(h), :],
            ru_s.at[t, h], ru_r.at[t, h], at_z(up_z),
        )

    def chip_sum(o, h):
        return own[o, part(h), :] + sib_recv[o, part(h), :].astype(F32)

    for t in range(nd):
        o_dn, o_up = (z + n_z - nd + t) % n_z, (z + nu - t + n_z) % n_z
        pt_copy(o_dn).wait_recv()
        pt_copy(o_up).wait_recv()
        for h in range(SUM_PIECES):
            total = chip_sum(o_dn, h)
            if t > 0:
                rd_copy(t - 1, h).wait_recv()
                total += dn_recv[t - 1, part(h), :].astype(F32)
            dn_send[t, part(h), :] = total.astype(BF16)
            rd_copy(t, h).start()
            if t < nu:
                total = chip_sum(o_up, h)
                if t > 0:
                    ru_copy(t - 1, h).wait_recv()
                    total += up_recv[t - 1, part(h), :].astype(F32)
                up_send[t, part(h), :] = total.astype(BF16)
                ru_copy(t, h).start()
            for _ in range(1 if n_z == 16 else len(work)):
                if work:
                    work.pop(0)()
        if t == nd - 2:
            small_middle()

    small_end()
    for h in range(SUM_PIECES):
        total = chip_sum(z, h)
        ru_copy(nu - 1, h).wait_recv()
        total += up_recv[nu - 1, part(h), :].astype(F32)
        rd_copy(nd - 1, h).wait_recv()
        total += dn_recv[nd - 1, part(h), :].astype(F32)
        fin[part(h), :] = total.astype(BF16)

    per_core = n_ep // 2
    own_core = e // per_core

    def fa_copy(i, to, sender):
        return remote(
            fin.at[pl.ds(i * cap, cap), :], gat.at[block(sender), :],
            fa_s.at[i], fa_r.at[sender], (to, z * 2 + GATHER_CORE),
        )

    def stays(b):
        return (b == e) & (c == GATHER_CORE)

    def fa_local(i):
        return pltpu.make_async_copy(
            fin.at[pl.ds(i * cap, cap), :], gat.at[block(e), :], loc_sem.at[1]
        )

    for i in range(per_core):
        b = c * per_core + i

        @pl.when(jnp.logical_not(stays(b)))
        def _():
            fa_copy(i, b, e).start()

        @pl.when(stays(b))
        def _():
            fa_local(i).start()

    piece = tok // GATHER_PIECES

    def chunk(o, h):
        return tg.at[pl.ds(h * piece, piece), pl.ds(pl.multiple_of(o * LANES, LANES), LANES)]

    def au_copy(t, h, o):
        ref = chunk(o, h)
        return remote(ref, ref, au_s.at[t, h], au_r.at[t, h], at_z(up_z))

    def ad_copy(t, h, o):
        ref = chunk(o, h)
        return remote(ref, ref, ad_s.at[t, h], ad_r.at[t, h], at_z(dn_z))

    def as_copy(o, h):
        ref = chunk(o, h)
        return remote(ref, ref, as_s.at[o, h], as_r.at[o, h], sibling)

    @pl.when(c == GATHER_CORE)
    def _():
        @pl.when(own_core == GATHER_CORE)
        def _():
            fa_local(0).wait()

        @pl.when(own_core != GATHER_CORE)
        def _():
            fa_copy(0, e, e).wait_recv()

        @pl.loop(1, n_ep)
        def _(j):
            s = (e + j) % n_ep
            fa_copy(0, s, s).wait_recv()

        for h in range(GATHER_PIECES):
            at = slice(h * piece, (h + 1) * piece)
            acc = jnp.dot(pickt[at, :], gat[...], preferred_element_type=F32)
            tg[at, pl.ds(pl.multiple_of(z * LANES, LANES), LANES)] = acc.astype(BF16)
            au_copy(1, h, z).start()
            ad_copy(1, h, z).start()
            as_copy(z, h).start()
        for t in range(1, nd + 1):
            for h in range(GATHER_PIECES):
                if t <= nu:
                    o = (z + n_z - t) % n_z
                    au_copy(t, h, o).wait_recv()
                    if t < nu:
                        au_copy(t + 1, h, o).start()
                    as_copy(o, h).start()
                o = (z + t) % n_z
                ad_copy(t, h, o).wait_recv()
                if t < nd:
                    ad_copy(t + 1, h, o).start()
                as_copy(o, h).start()

    @pl.loop(1, n_z)
    def _(j):
        o = (z + j) % n_z
        mg_copy(o, o).wait_recv()

    units = float(LANES * 2 * n_z)
    for o in range(n_z):
        gn_out[:, o * LANES : (o + 1) * LANES] = sm_fin[o, :, :LANES] / units
        un_out[:, o * LANES : (o + 1) * LANES] = sm_fin[o, :, LANES : 2 * LANES] / units
    dn_out[...] = lax.dot_general(
        jnp.ones((8, LANES), F32), dnacc[...], CONTRACT_LAST,
        precision=lax.Precision.HIGHEST, preferred_element_type=F32,
    )[0:1, :] / float(LANES * n_z)
    for h in range(score_rows):
        at = slice(h * LANES, (h + 1) * LANES)
        gp = gp_ref[:, at]
        total = jnp.zeros((1, LANES), F32)
        for k in range(2):
            ep = ep_ref[k : k + 1, at]
            score = sm_fin[k * score_rows + h, :, 2 * LANES :] / (gp * ep)
            epg_out[k : k + 1, at] = gp * score
            total += ep * score
        gpg_out[:, at] = total

    @pl.when(c != GATHER_CORE)
    def _():
        @pl.loop(0, n_z)
        def _(o):
            for h in range(GATHER_PIECES):
                as_copy(o, h).wait_recv()

    tg_store = pltpu.make_async_copy(tg, tg_out, out_sem.at[3])
    tg_store.start()

    for copy in grad_stores():
        copy.wait()

    @pl.loop(1, n_ep)
    def _(j):
        p = plane_peer(e, j, n_ep)
        in_copy(p, p, e).wait_send()
        sc_copy(p, e).wait_send()

    @pl.loop(0, n_ep)
    def _(s):
        za_copy(s, mine).wait_send()
        zb_copy(s, mine).wait_send()
        dx_copy(s, c).wait_send()
        dy_copy(s, c).wait_send()

    @pl.loop(0, n_z)
    def _(o):
        pt_copy(o).wait_send()

    @pl.loop(1, n_z)
    def _(j):
        o = (z + j) % n_z
        ms_copy(o, z).wait_send()
        mg_copy(z, o).wait_send()

    mx_copy().wait_send()
    for h in range(SUM_PIECES):
        for t in range(nd):
            rd_copy(t, h).wait_send()
        for t in range(nu):
            ru_copy(t, h).wait_send()

    for i in range(per_core):
        b = c * per_core + i

        @pl.when(jnp.logical_not(stays(b)))
        def _():
            fa_copy(i, b, e).wait_send()

    @pl.when(c == GATHER_CORE)
    def _():
        for h in range(GATHER_PIECES):
            for t in range(1, nu + 1):
                au_copy(t, h, z).wait_send()
            for t in range(1, nd + 1):
                ad_copy(t, h, z).wait_send()

            @pl.loop(0, n_z)
            def _(o):
                as_copy(o, h).wait_send()

    tg_store.wait()


def flush(count, *refs):
    ins, outs, bufs = refs[:count], refs[count : 2 * count], refs[2 * count : 3 * count]
    in_sem, out_sem = refs[3 * count :]
    reads = [pltpu.make_async_copy(ins[i], bufs[i], in_sem.at[i]) for i in range(count)]
    writes = [pltpu.make_async_copy(bufs[i], outs[i], out_sem.at[i]) for i in range(count)]
    for copy in reads:
        copy.start()
    for i in range(count):
        reads[i].wait()
        writes[i].start()
    for copy in writes:
        copy.wait()


def write_out(arrays):
    count = len(arrays)
    any_spec = pl.BlockSpec(memory_space=pl.ANY)
    return pl.pallas_call(
        functools.partial(flush, count),
        out_shape=tuple(jax.ShapeDtypeStruct(a.shape, a.dtype) for a in arrays),
        in_specs=[any_spec] * count,
        out_specs=(any_spec,) * count,
        scratch_shapes=[pltpu.VMEM(a.shape, a.dtype) for a in arrays]
        + [pltpu.SemaphoreType.DMA((count,)), pltpu.SemaphoreType.DMA((count,))],
    )(*arrays)


def local(tokens, cotangent, group_prob, expert_prob, routing, gate_weight, up_weight, down_weight):
    tok, width = tokens.shape
    n_ep = lax.axis_size("ep")
    n_z = lax.axis_size("tp") // 2
    cap = 3 * tok * 2 // (2 * n_ep)
    slots = n_ep * cap
    half = slots // 2
    quarter = width // 4
    unit = gate_weight.shape[2]
    nd, nu = n_z // 2, n_z // 2 - 1
    scw = -(-cap // LANES) * LANES
    dma = pltpu.SemaphoreType.DMA
    vm = pltpu.VMEM
    any_spec = pl.BlockSpec(memory_space=pl.ANY)
    vm_spec = pl.BlockSpec(memory_space=pltpu.VMEM)
    outs = pl.pallas_call(
        functools.partial(body, n_ep, n_z, cap),
        out_shape=(
            jax.ShapeDtypeStruct((tok, width), BF16),
            jax.ShapeDtypeStruct((1, width, unit), BF16),
            jax.ShapeDtypeStruct((1, width, unit), BF16),
            jax.ShapeDtypeStruct((1, unit, width), BF16),
            jax.ShapeDtypeStruct((1, width), F32),
            jax.ShapeDtypeStruct((1, width), F32),
            jax.ShapeDtypeStruct((1, unit), F32),
            jax.ShapeDtypeStruct((2, tok), F32),
            jax.ShapeDtypeStruct((1, tok), F32),
        ),
        in_specs=[vm_spec] * 3 + [any_spec] * 5,
        out_specs=(any_spec,) * 4 + (vm_spec,) * 5,
        scratch_shapes=[
            vm((tok, 2 * quarter), BF16),
            vm((2, slots, quarter), BF16),
            vm((2, 4, slots, quarter), BF16),
            vm((4, quarter, 2 * unit), BF16),
            vm((4, unit, quarter), BF16),
            vm((slots, 2 * unit), F32),
            vm((slots, unit), F32),
            vm((slots, 2 * unit), BF16),
            vm((2 * unit, slots), BF16),
            vm((unit, slots), BF16),
            vm((slots, unit), F32),
            vm((n_z, half, LANES), F32),
            vm((n_z, half, LANES), BF16),
            vm((n_z, half, LANES), BF16),
            vm((nd, half, LANES), BF16),
            vm((nd, half, LANES), BF16),
            vm((nu, half, LANES), BF16),
            vm((nu, half, LANES), BF16),
            vm((n_ep, 1, scw), F32),
            vm((n_ep, 1, scw), F32),
            vm((n_z, 1, 3 * LANES), F32),
            vm((n_z, 1, 3 * LANES), F32),
            vm((1, 3 * LANES), F32),
            vm((1, 3 * LANES), F32),
            vm((n_z, 1, 3 * LANES), F32),
            vm((half, LANES), BF16),
            vm((slots, LANES), BF16),
            vm((tok, width), BF16),
            vm((width, unit), BF16),
            vm((width, unit), BF16),
            vm((unit, width), BF16),
            vm((unit, LANES), F32),
            dma, dma((4, 3)), dma((2,)),
            dma((n_ep,)), dma((n_ep,)), dma((n_ep,)), dma((n_ep,)), dma((n_ep,)), dma((n_ep,)),
            dma((n_ep,)), dma((n_ep,)), dma((n_ep,)), dma((n_ep,)),
            dma((n_ep,)), dma((n_ep,)),
            dma((n_z,)), dma((n_z,)),
            dma((nd, SUM_PIECES)), dma((nd, SUM_PIECES)), dma((nu, SUM_PIECES)), dma((nu, SUM_PIECES)),
            dma((n_z,)), dma((n_z,)), dma((1,)), dma((1,)), dma((n_z,)), dma((n_z,)),
            dma((n_ep // 2,)), dma((n_ep,)),
            dma((nu + 1, GATHER_PIECES)), dma((nu + 1, GATHER_PIECES)),
            dma((nd + 1, GATHER_PIECES)), dma((nd + 1, GATHER_PIECES)),
            dma((n_z, GATHER_PIECES)), dma((n_z, GATHER_PIECES)),
            dma((4,)), pltpu.SemaphoreType.REGULAR, pltpu.SemaphoreType.REGULAR,
            vm((tok, slots), BF16),
        ],
        compiler_params=pltpu.CompilerParams(
            collective_id=0, has_side_effects=True, vmem_limit_bytes=56 * 1024 * 1024
        ),
    )(
        routing.T, group_prob[None, :], expert_prob.T, tokens, cotangent,
        gate_weight, up_weight, down_weight,
    )
    tg, gg, ug, dg, gn, un, dn, epg, gpg = write_out(outs)
    return tg, gpg[0], epg.T, gg, ug, dg, gn, un, dn


def solution(mesh):
    return jax.shard_map(
        local,
        mesh=mesh,
        in_specs=(
            P("ep", None),
            P("ep", None),
            P("ep"),
            P("ep", None),
            P("ep", None),
            P("ep", None, "tp"),
            P("ep", None, "tp"),
            P("ep", "tp", None),
        ),
        out_specs=(
            P("ep", None),
            P("ep"),
            P("ep", None),
            P("ep", None, "tp"),
            P("ep", None, "tp"),
            P("ep", "tp", None),
            P("ep", None),
            P("ep", None),
            P("ep", "tp"),
        ),
        check_vma=False,
    )
```

```python
import functools
import jax
import jax.numpy as jnp
from jax import lax
from jax.experimental import pallas as pl
from jax.experimental.pallas import tpu as pltpu
from jax.sharding import PartitionSpec as P

MESH = pl.DeviceIdType.MESH
LANES = 128
F32 = jnp.float32
BF16 = jnp.bfloat16
CONTRACT_LAST = (((1,), (1,)), ((), ()))
SUM_PIECES = 4
GATHER_PIECES = 2
CHAIN_CORE = 1


def plane_peer(e, j, n_ep):
    if n_ep == 16:
        y, x = e // 4, e % 4
        return ((y + j // 4) % 4) * 4 + (x + j % 4) % 4
    return (e + j) % n_ep


def plane_source(e, j, n_ep):
    if n_ep == 16:
        y, x = e // 4, e % 4
        return ((y + 4 - j // 4) % 4) * 4 + (x + 4 - j % 4) % 4
    return (e + n_ep - j) % n_ep


def slot_rows(r, n_ep, cap):
    tok = r.shape[1]
    names = lax.broadcasted_iota(jnp.int32, (n_ep, tok), 0)
    first = (names == r[0:1, :]).astype(F32)
    second = (names == r[1:2, :]).astype(F32)
    earlier = lax.broadcasted_iota(jnp.int32, (tok, tok), 0) < lax.broadcasted_iota(
        jnp.int32, (tok, tok), 1
    )
    before = jnp.dot(
        (first + second).astype(BF16),
        jnp.where(earlier, 1.0, 0.0).astype(BF16),
        preferred_element_type=F32,
    )
    out = []
    for k, hot in enumerate((first, second)):
        place = jnp.sum(hot * before, axis=0, keepdims=True)
        out.append(r[k : k + 1, :].astype(F32) * float(cap) + place)
    return out


def body(
    n_ep, n_z, cap,
    r_ref, gp_ref, ep_ref, tok_hbm, cot_hbm, wg_hbm, wu_hbm, wd_hbm,
    tg_out, gg_out, ug_out, dg_out, gn_out, un_out, dn_out, epg_out, gpg_out,
    x, send, rows, wgu, wd, pre, hg, gpu, gput, hidt, prod,
    own, sib_send, sib_recv, dn_send, dn_recv, up_send, up_recv,
    sc_send, sc_recv, sm, sm_recv, sm_tot, sm_sib, sm_fin,
    fin, gat, tg, gg, ug, dg, dnacc,
    ld_sem, wl_sem, loc_sem, in_s, in_r, za_s, za_r, zb_s, zb_r, dx_s, dx_r, dy_s, dy_r,
    sc_s, sc_r, pt_s, pt_r, rd_s, rd_r, ru_s, ru_r, ms_s, ms_r, mx_s, mx_r, mg_s, mg_r,
    fa_s, fa_r, au_s, au_r, ad_s, ad_r, as_s, as_r, out_sem, met4, met8, pickt,
):
    e, tp = lax.axis_index("ep"), lax.axis_index("tp")
    z, c = tp // 2, tp % 2
    par = z % 2
    mine, other = par * 2, 2 - par * 2
    near, far = z + 1 - 2 * par, (z + n_z - 1 + 2 * par) % n_z
    up_z, dn_z = (z + 1) % n_z, (z + n_z - 1) % n_z
    tok, quarter = x.shape[0], rows.shape[3]
    slots = n_ep * cap
    nd, nu = n_z // 2, n_z // 2 - 1
    qc = quarter // LANES
    sibling = (e, z * 2 + 1 - c)

    def at_z(other_z):
        return (e, other_z * 2 + c)

    def remote(src, dst, s_sem, r_sem, dev):
        return pltpu.make_async_remote_copy(
            src_ref=src, dst_ref=dst, send_sem=s_sem, recv_sem=r_sem,
            device_id=dev, device_id_type=MESH,
        )

    barrier = pltpu.get_barrier_semaphore()

    @pl.loop(1, n_ep)
    def _(j):
        pl.semaphore_signal(
            barrier, inc=1, device_id=(plane_peer(e, j, n_ep), tp), device_id_type=MESH
        )

    for step in (1, 2):
        for o in (z + step, z + n_z - step):
            pl.semaphore_signal(barrier, inc=1, device_id=at_z(o % n_z), device_id_type=MESH)
    pl.semaphore_signal(barrier, inc=1, device_id=sibling, device_id_type=MESH)

    def greet(sem, step):
        for o in (z + step, z + n_z - step):
            pl.semaphore_signal(sem, inc=1, device_id=at_z(o % n_z), device_id_type=MESH)

    start_col = pl.multiple_of(par * (2 * quarter), LANES)

    @pl.when(c == 0)
    def _():
        pltpu.make_async_copy(tok_hbm.at[:, pl.ds(start_col, 2 * quarter)], x, ld_sem).start()

    @pl.when(c == 1)
    def _():
        pltpu.make_async_copy(cot_hbm.at[:, pl.ds(start_col, 2 * quarter)], x, ld_sem).start()

    def weight_loads():
        out = []
        for q in range(4):
            span = pl.ds(q * quarter, quarter)
            out.append((wg_hbm.at[0, span, :], wgu.at[q, :, pl.ds(0, LANES)], wl_sem.at[q, 0]))
            out.append((wu_hbm.at[0, span, :], wgu.at[q, :, pl.ds(LANES, LANES)], wl_sem.at[q, 1]))
            out.append((wd_hbm.at[0, :, span], wd.at[q], wl_sem.at[q, 2]))
        return [pltpu.make_async_copy(*args) for args in out]

    for copy in weight_loads():
        copy.start()

    r = r_ref[...]
    weight = gp_ref[...] * ep_ref[...]
    w_eff = jnp.where(c == 0, jnp.ones_like(weight), weight)
    slot0, slot1 = slot_rows(r, n_ep, cap)
    pltpu.make_async_copy(tok_hbm.at[:, pl.ds(start_col, 2 * quarter)], x, ld_sem).wait()

    @pl.loop(0, slots // LANES)
    def _(i):
        at = pl.multiple_of(i * LANES, LANES)
        here = (lax.broadcasted_iota(jnp.int32, (LANES, tok), 0) + at).astype(F32)
        m0, m1 = here == slot0, here == slot1
        pick = jnp.where(m0 | m1, 1.0, 0.0).astype(BF16)
        scale = jnp.sum(
            jnp.where(m0, w_eff[0:1, :], 0.0) + jnp.where(m1, w_eff[1:2, :], 0.0),
            axis=1, keepdims=True,
        )
        got = scale * jnp.dot(pick, x[...], preferred_element_type=F32)
        send[0, pl.ds(at, LANES), :] = got[:, :quarter].astype(BF16)
        send[1, pl.ds(at, LANES), :] = got[:, quarter:].astype(BF16)

    pre[...] = jnp.zeros_like(pre)
    hg[...] = jnp.zeros_like(hg)
    pl.semaphore_wait(barrier, n_ep - 1 + 4 + 1)
    greet(met4, 2)

    def block(b):
        return pl.ds(pl.multiple_of(b * cap, 16), cap)

    def own_block():
        return pltpu.make_async_copy(
            send.at[:, block(e), :], rows.at[c, pl.ds(mine, 2), block(e), :], loc_sem.at[0]
        )

    def in_copy(src_block, to, sender):
        return remote(
            send.at[:, block(src_block), :], rows.at[c, pl.ds(mine, 2), block(sender), :],
            in_s.at[src_block], in_r.at[sender], (to, tp),
        )

    def za_copy(s, first):
        ref = rows.at[c, first, block(s), :]
        return remote(ref, ref, za_s.at[s], za_r.at[s], at_z(near))

    def zb_copy(s, first):
        ref = rows.at[c, first + 1, block(s), :]
        return remote(ref, ref, zb_s.at[s], zb_r.at[s], at_z(far))

    def dx_copy(s, arr):
        ref = rows.at[arr, pl.ds(mine, 2), block(s), :]
        return remote(ref, ref, dx_s.at[s], dx_r.at[s], sibling)

    def dy_copy(s, arr):
        ref = rows.at[arr, pl.ds(other, 2), block(s), :]
        return remote(ref, ref, dy_s.at[s], dy_r.at[s], sibling)

    own_block().start()

    @pl.loop(1, n_ep)
    def _(j):
        p = plane_peer(e, j, n_ep)
        in_copy(p, p, e).start()

    own_block().wait()
    za_copy(e, mine).start()
    zb_copy(e, mine).start()
    dx_copy(e, c).start()

    @pl.loop(1, n_ep)
    def _(j):
        s = plane_source(e, j, n_ep)
        in_copy(s, s, s).wait_recv()
        za_copy(s, mine).start()
        zb_copy(s, mine).start()
        dx_copy(s, c).start()

    def gate_up_part(q):
        pre[...] += jnp.dot(rows[0, q], wgu[q], preferred_element_type=F32)

    def down_part(q):
        hg[...] += lax.dot_general(rows[1, q], wd[q], CONTRACT_LAST, preferred_element_type=F32)

    def multiply(first, arr_is_own):
        is_in = (c == 0) if arr_is_own else (c == 1)

        @pl.when(is_in)
        def _():
            @pl.loop(0, 2)
            def _(i):
                gate_up_part(first + i)

        @pl.when(jnp.logical_not(is_in))
        def _():
            @pl.loop(0, 2)
            def _(i):
                down_part(first + i)

    for copy in weight_loads():
        copy.wait()
    pl.semaphore_wait(met4, 2)
    greet(met8, 4)
    multiply(mine, True)

    @pl.loop(0, n_ep)
    def _(j):
        s = plane_source(e, j, n_ep)
        za_copy(s, other).wait_recv()
        zb_copy(s, other).wait_recv()
        dy_copy(s, c).start()

    multiply(other, True)

    @pl.loop(0, n_ep)
    def _(j):
        dx_copy(plane_source(e, j, n_ep), 1 - c).wait_recv()

    multiply(mine, False)

    @pl.loop(0, n_ep)
    def _(j):
        dy_copy(plane_source(e, j, n_ep), 1 - c).wait_recv()

    pl.semaphore_wait(met8, 2)
    multiply(other, False)

    @pl.loop(0, slots // LANES)
    def _(i):
        at = pl.ds(pl.multiple_of(i * LANES, LANES), LANES)
        gate, upv, grad = pre[at, :LANES], pre[at, LANES:], hg[at, :]
        sigma = jax.nn.sigmoid(gate)
        activated = gate * sigma
        derivative = sigma * (1.0 + gate * (1.0 - sigma))
        hidden = (activated * upv).astype(BF16).astype(F32)
        gate_pre = (grad * upv * derivative).astype(BF16).astype(F32)
        up_pre = (grad * activated).astype(BF16).astype(F32)
        prod[at, :] = hidden * grad
        gpu[at, :LANES] = gate_pre.astype(BF16)
        gpu[at, LANES:] = up_pre.astype(BF16)
        gput[:LANES, at] = gate_pre.T.astype(BF16)
        gput[LANES:, at] = up_pre.T.astype(BF16)
        hidt[:, at] = hidden.T.astype(BF16)

    def sc_copy(to, sender):
        return remote(sc_send.at[to], sc_recv.at[sender], sc_s.at[to], sc_r.at[sender], (to, tp))

    def pt_copy(o):
        return remote(sib_send.at[o], sib_recv.at[o], pt_s.at[o], pt_r.at[o], sibling)

    def input_part(q):
        return lax.dot_general(gpu[...], wgu[q], CONTRACT_LAST, preferred_element_type=F32)

    def quarters():
        return [((z + nd) // qc + step) % 4 for step in (0, 3, 1, 2)]

    @pl.when(c != CHAIN_CORE)
    def _():
        for q in quarters():
            part = input_part(q)
            for i in range(qc):
                sib_send[q * qc + i] = part[:, i * LANES : (i + 1) * LANES].astype(BF16)
                pt_copy(q * qc + i).start()

    @pl.when(c == CHAIN_CORE)
    def _():
        for q in quarters():
            part = input_part(q)
            for i in range(qc):
                own[q * qc + i] = part[:, i * LANES : (i + 1) * LANES]

    dnacc[...] = jnp.zeros_like(dnacc)

    def down_piece(q):
        down = jnp.dot(hidt[...], rows[1, q], preferred_element_type=F32)
        dg[:, q * quarter : (q + 1) * quarter] = down.astype(BF16)
        square = down * down
        dnacc[...] += sum(square[:, i * LANES : (i + 1) * LANES] for i in range(qc))

    def in_piece(k, q):
        target = (gg, ug)[k]
        both = jnp.dot(gput[k * LANES : (k + 1) * LANES, :], rows[0, q], preferred_element_type=F32)
        norm = jnp.sum(both * both, axis=0, keepdims=True)
        for i in range(qc):
            sm[q * qc + i, :, k * LANES : (k + 1) * LANES] = norm[:, i * LANES : (i + 1) * LANES]
        target[q * quarter : (q + 1) * quarter, :] = both.T.astype(BF16)

    def pick_piece():
        lane = lax.broadcasted_iota(jnp.int32, (slots, tok), 0).astype(F32)
        pick = jnp.where((lane == slot0) | (lane == slot1), 1.0, 0.0)
        pickt[...] = pick.T.astype(BF16)

    def grad_stores():
        return [
            pltpu.make_async_copy(gg, gg_out.at[0], out_sem.at[0]),
            pltpu.make_async_copy(ug, ug_out.at[0], out_sem.at[1]),
            pltpu.make_async_copy(dg, dg_out.at[0], out_sem.at[2]),
        ]

    def own_scores():
        sc_recv[e] = sc_send[e]

    def ms_copy(o, sender):
        return remote(sm.at[o], sm_recv.at[sender], ms_s.at[o], ms_r.at[sender], at_z(o))

    def mx_copy():
        return remote(sm_tot, sm_sib, mx_s.at[0], mx_r.at[0], sibling)

    def mg_copy(piece, to):
        return remote(sm_fin.at[piece], sm_fin.at[piece], mg_s.at[to], mg_r.at[piece], at_z(to))

    score_rows = tok // LANES

    def small_start():
        own_scores()

        @pl.loop(1, n_ep)
        def _(j):
            s = plane_source(e, j, n_ep)
            sc_copy(s, s).wait_recv()

        got = sc_recv[...].reshape(n_ep, sc_recv.shape[2])
        fill = jnp.zeros((LANES - n_ep, got.shape[1]), F32)
        columns = jnp.concatenate([got, fill], axis=0).T
        totals = [jnp.zeros((1, tok), F32), jnp.zeros((1, tok), F32)]
        lane = lax.broadcasted_iota(jnp.int32, (cap, tok), 0)
        for s in range(n_ep):
            here = (lane + s * cap).astype(F32)
            column = columns[:cap, s : s + 1]
            for k, slot in enumerate((slot0, slot1)):
                totals[k] += jnp.sum(jnp.where(here == slot, column, 0.0), axis=0, keepdims=True)
        sm[:, :, 2 * LANES :] = jnp.zeros((n_z, 1, LANES), F32)
        for k in range(2):
            for h in range(score_rows):
                sm[k * score_rows + h, :, 2 * LANES :] = totals[k][:, h * LANES : (h + 1) * LANES]

        @pl.loop(1, n_z)
        def _(j):
            o = (z + j) % n_z
            ms_copy(o, z).start()

    def small_middle():
        @pl.loop(1, n_z)
        def _(j):
            s = (z + j) % n_z
            ms_copy(s, s).wait_recv()

        sm_recv[z] = sm[z]
        sm_tot[...] = jnp.sum(sm_recv[...], axis=0)
        mx_copy().start()

    def small_end():
        mx_copy().wait_recv()
        sm_fin[z] = sm_tot[...] + sm_sib[...]

        @pl.loop(1, n_z)
        def _(j):
            mg_copy(z, (z + j) % n_z).start()

    def scores():
        ones = jnp.ones((8, LANES), F32)
        for b in range(n_ep):
            row = lax.dot_general(
                ones, prod[b * cap : (b + 1) * cap, :], CONTRACT_LAST,
                precision=lax.Precision.HIGHEST, preferred_element_type=F32,
            )
            sc_send[b, :, :cap] = row[0:1, :]

        @pl.loop(1, n_ep)
        def _(j):
            p = plane_peer(e, j, n_ep)
            sc_copy(p, e).start()

    def store_start():
        for copy in grad_stores():
            copy.start()

    work = [scores]
    for q in range(4):
        work += [functools.partial(down_piece, q)]
        work += [functools.partial(in_piece, 0, q), functools.partial(in_piece, 1, q)]
    work += [small_start, store_start]

    sub = slots // SUM_PIECES

    def part(h):
        return pl.ds(h * sub, sub)

    def rd_copy(t, h):
        return remote(
            dn_send.at[t, part(h), :], dn_recv.at[t, part(h), :],
            rd_s.at[t, h], rd_r.at[t, h], at_z(dn_z),
        )

    def ru_copy(t, h):
        return remote(
            up_send.at[t, part(h), :], up_recv.at[t, part(h), :],
            ru_s.at[t, h], ru_r.at[t, h], at_z(up_z),
        )

    def chip_sum(o, h):
        return own[o, part(h), :] + sib_recv[o, part(h), :].astype(F32)

    @pl.when(c != CHAIN_CORE)
    def _():
        for step in work:
            step()
        small_middle()
        small_end()

    @pl.when(c == CHAIN_CORE)
    def _():
        todo = work + [pick_piece]
        for t in range(nd):
            o_dn, o_up = (z + n_z - nd + t) % n_z, (z + nu - t + n_z) % n_z
            pt_copy(o_dn).wait_recv()
            pt_copy(o_up).wait_recv()
            for h in range(SUM_PIECES):
                total = chip_sum(o_dn, h)
                if t > 0:
                    rd_copy(t - 1, h).wait_recv()
                    total += dn_recv[t - 1, part(h), :].astype(F32)
                dn_send[t, part(h), :] = total.astype(BF16)
                rd_copy(t, h).start()
                if t < nu:
                    total = chip_sum(o_up, h)
                    if t > 0:
                        ru_copy(t - 1, h).wait_recv()
                        total += up_recv[t - 1, part(h), :].astype(F32)
                    up_send[t, part(h), :] = total.astype(BF16)
                    ru_copy(t, h).start()
                for _ in range(1 if n_z == 16 else len(todo)):
                    if todo:
                        todo.pop(0)()
            if t == nd - 2:
                small_middle()

        small_end()
        for h in range(SUM_PIECES):
            total = chip_sum(z, h)
            ru_copy(nu - 1, h).wait_recv()
            total += up_recv[nu - 1, part(h), :].astype(F32)
            rd_copy(nd - 1, h).wait_recv()
            total += dn_recv[nd - 1, part(h), :].astype(F32)
            fin[part(h), :] = total.astype(BF16)

    def fa_copy(b, sender):
        return remote(
            fin.at[block(b), :], gat.at[block(sender), :], fa_s.at[b], fa_r.at[sender], (b, tp)
        )

    def fa_local():
        return pltpu.make_async_copy(fin.at[block(e), :], gat.at[block(e), :], loc_sem.at[1])

    piece = tok // GATHER_PIECES

    def chunk(o, h):
        return tg.at[pl.ds(h * piece, piece), pl.ds(pl.multiple_of(o * LANES, LANES), LANES)]

    def au_copy(t, h, o):
        ref = chunk(o, h)
        return remote(ref, ref, au_s.at[t, h], au_r.at[t, h], at_z(up_z))

    def ad_copy(t, h, o):
        ref = chunk(o, h)
        return remote(ref, ref, ad_s.at[t, h], ad_r.at[t, h], at_z(dn_z))

    def as_copy(o, h):
        ref = chunk(o, h)
        return remote(ref, ref, as_s.at[o, h], as_r.at[o, h], sibling)

    @pl.when(c == CHAIN_CORE)
    def _():
        fa_local().start()

        @pl.loop(1, n_ep)
        def _(j):
            fa_copy(plane_peer(e, j, n_ep), e).start()

        fa_local().wait()

        @pl.loop(1, n_ep)
        def _(j):
            s = plane_source(e, j, n_ep)
            fa_copy(s, s).wait_recv()

        for h in range(GATHER_PIECES):
            at = slice(h * piece, (h + 1) * piece)
            acc = jnp.dot(pickt[at, :], gat[...], preferred_element_type=F32)
            tg[at, pl.ds(pl.multiple_of(z * LANES, LANES), LANES)] = acc.astype(BF16)
            au_copy(1, h, z).start()
            ad_copy(1, h, z).start()
            as_copy(z, h).start()
        for t in range(1, nd + 1):
            for h in range(GATHER_PIECES):
                if t <= nu:
                    o = (z + n_z - t) % n_z
                    au_copy(t, h, o).wait_recv()
                    if t < nu:
                        au_copy(t + 1, h, o).start()
                    as_copy(o, h).start()
                o = (z + t) % n_z
                ad_copy(t, h, o).wait_recv()
                if t < nd:
                    ad_copy(t + 1, h, o).start()
                as_copy(o, h).start()

    @pl.loop(1, n_z)
    def _(j):
        o = (z + j) % n_z
        mg_copy(o, o).wait_recv()

    units = float(LANES * 2 * n_z)
    for o in range(n_z):
        gn_out[:, o * LANES : (o + 1) * LANES] = sm_fin[o, :, :LANES] / units
        un_out[:, o * LANES : (o + 1) * LANES] = sm_fin[o, :, LANES : 2 * LANES] / units
    dn_out[...] = lax.dot_general(
        jnp.ones((8, LANES), F32), dnacc[...], CONTRACT_LAST,
        precision=lax.Precision.HIGHEST, preferred_element_type=F32,
    )[0:1, :] / float(LANES * n_z)
    for h in range(score_rows):
        at = slice(h * LANES, (h + 1) * LANES)
        gp = gp_ref[:, at]
        total = jnp.zeros((1, LANES), F32)
        for k in range(2):
            ep = ep_ref[k : k + 1, at]
            score = sm_fin[k * score_rows + h, :, 2 * LANES :] / (gp * ep)
            epg_out[k : k + 1, at] = gp * score
            total += ep * score
        gpg_out[:, at] = total

    @pl.when(c != CHAIN_CORE)
    def _():
        @pl.loop(0, n_z)
        def _(o):
            for h in range(GATHER_PIECES):
                as_copy(o, h).wait_recv()

    tg_store = pltpu.make_async_copy(tg, tg_out, out_sem.at[3])
    tg_store.start()

    for copy in grad_stores():
        copy.wait()

    @pl.loop(1, n_ep)
    def _(j):
        p = plane_peer(e, j, n_ep)
        in_copy(p, p, e).wait_send()
        sc_copy(p, e).wait_send()

    @pl.loop(0, n_ep)
    def _(s):
        za_copy(s, mine).wait_send()
        zb_copy(s, mine).wait_send()
        dx_copy(s, c).wait_send()
        dy_copy(s, c).wait_send()

    @pl.loop(1, n_z)
    def _(j):
        o = (z + j) % n_z
        ms_copy(o, z).wait_send()
        mg_copy(z, o).wait_send()

    mx_copy().wait_send()
    @pl.when(c != CHAIN_CORE)
    def _():
        @pl.loop(0, n_z)
        def _(o):
            pt_copy(o).wait_send()

    @pl.when(c == CHAIN_CORE)
    def _():
        @pl.loop(1, n_ep)
        def _(j):
            fa_copy(plane_peer(e, j, n_ep), e).wait_send()

        for h in range(SUM_PIECES):
            for t in range(nd):
                rd_copy(t, h).wait_send()
            for t in range(nu):
                ru_copy(t, h).wait_send()

    @pl.when(c == CHAIN_CORE)
    def _():
        for h in range(GATHER_PIECES):
            for t in range(1, nu + 1):
                au_copy(t, h, z).wait_send()
            for t in range(1, nd + 1):
                ad_copy(t, h, z).wait_send()

            @pl.loop(0, n_z)
            def _(o):
                as_copy(o, h).wait_send()

    tg_store.wait()


def flush(count, *refs):
    ins, outs, bufs = refs[:count], refs[count : 2 * count], refs[2 * count : 3 * count]
    in_sem, out_sem = refs[3 * count :]
    reads = [pltpu.make_async_copy(ins[i], bufs[i], in_sem.at[i]) for i in range(count)]
    writes = [pltpu.make_async_copy(bufs[i], outs[i], out_sem.at[i]) for i in range(count)]
    for copy in reads:
        copy.start()
    for i in range(count):
        reads[i].wait()
        writes[i].start()
    for copy in writes:
        copy.wait()


def write_out(arrays):
    count = len(arrays)
    any_spec = pl.BlockSpec(memory_space=pl.ANY)
    return pl.pallas_call(
        functools.partial(flush, count),
        out_shape=tuple(jax.ShapeDtypeStruct(a.shape, a.dtype) for a in arrays),
        in_specs=[any_spec] * count,
        out_specs=(any_spec,) * count,
        scratch_shapes=[pltpu.VMEM(a.shape, a.dtype) for a in arrays]
        + [pltpu.SemaphoreType.DMA((count,)), pltpu.SemaphoreType.DMA((count,))],
    )(*arrays)


def local(tokens, cotangent, group_prob, expert_prob, routing, gate_weight, up_weight, down_weight):
    tok, width = tokens.shape
    n_ep = lax.axis_size("ep")
    n_z = lax.axis_size("tp") // 2
    cap = 3 * tok * 2 // (2 * n_ep)
    slots = n_ep * cap
    quarter = width // 4
    unit = gate_weight.shape[2]
    nd, nu = n_z // 2, n_z // 2 - 1
    scw = -(-cap // LANES) * LANES
    dma = pltpu.SemaphoreType.DMA
    vm = pltpu.VMEM
    any_spec = pl.BlockSpec(memory_space=pl.ANY)
    vm_spec = pl.BlockSpec(memory_space=pltpu.VMEM)
    outs = pl.pallas_call(
        functools.partial(body, n_ep, n_z, cap),
        out_shape=(
            jax.ShapeDtypeStruct((tok, width), BF16),
            jax.ShapeDtypeStruct((1, width, unit), BF16),
            jax.ShapeDtypeStruct((1, width, unit), BF16),
            jax.ShapeDtypeStruct((1, unit, width), BF16),
            jax.ShapeDtypeStruct((1, width), F32),
            jax.ShapeDtypeStruct((1, width), F32),
            jax.ShapeDtypeStruct((1, unit), F32),
            jax.ShapeDtypeStruct((2, tok), F32),
            jax.ShapeDtypeStruct((1, tok), F32),
        ),
        in_specs=[vm_spec] * 3 + [any_spec] * 5,
        out_specs=(any_spec,) * 4 + (vm_spec,) * 5,
        scratch_shapes=[
            vm((tok, 2 * quarter), BF16),
            vm((2, slots, quarter), BF16),
            vm((2, 4, slots, quarter), BF16),
            vm((4, quarter, 2 * unit), BF16),
            vm((4, unit, quarter), BF16),
            vm((slots, 2 * unit), F32),
            vm((slots, unit), F32),
            vm((slots, 2 * unit), BF16),
            vm((2 * unit, slots), BF16),
            vm((unit, slots), BF16),
            vm((slots, unit), F32),
            vm((n_z, slots, LANES), F32),
            vm((n_z, slots, LANES), BF16),
            vm((n_z, slots, LANES), BF16),
            vm((nd, slots, LANES), BF16),
            vm((nd, slots, LANES), BF16),
            vm((nu, slots, LANES), BF16),
            vm((nu, slots, LANES), BF16),
            vm((n_ep, 1, scw), F32),
            vm((n_ep, 1, scw), F32),
            vm((n_z, 1, 3 * LANES), F32),
            vm((n_z, 1, 3 * LANES), F32),
            vm((1, 3 * LANES), F32),
            vm((1, 3 * LANES), F32),
            vm((n_z, 1, 3 * LANES), F32),
            vm((slots, LANES), BF16),
            vm((slots, LANES), BF16),
            vm((tok, width), BF16),
            vm((width, unit), BF16),
            vm((width, unit), BF16),
            vm((unit, width), BF16),
            vm((unit, LANES), F32),
            dma, dma((4, 3)), dma((2,)),
            dma((n_ep,)), dma((n_ep,)), dma((n_ep,)), dma((n_ep,)), dma((n_ep,)), dma((n_ep,)),
            dma((n_ep,)), dma((n_ep,)), dma((n_ep,)), dma((n_ep,)),
            dma((n_ep,)), dma((n_ep,)),
            dma((n_z,)), dma((n_z,)),
            dma((nd, SUM_PIECES)), dma((nd, SUM_PIECES)), dma((nu, SUM_PIECES)), dma((nu, SUM_PIECES)),
            dma((n_z,)), dma((n_z,)), dma((1,)), dma((1,)), dma((n_z,)), dma((n_z,)),
            dma((n_ep,)), dma((n_ep,)),
            dma((nu + 1, GATHER_PIECES)), dma((nu + 1, GATHER_PIECES)),
            dma((nd + 1, GATHER_PIECES)), dma((nd + 1, GATHER_PIECES)),
            dma((n_z, GATHER_PIECES)), dma((n_z, GATHER_PIECES)),
            dma((4,)), pltpu.SemaphoreType.REGULAR, pltpu.SemaphoreType.REGULAR,
            vm((tok, slots), BF16),
        ],
        compiler_params=pltpu.CompilerParams(
            collective_id=0, has_side_effects=True, vmem_limit_bytes=56 * 1024 * 1024
        ),
    )(
        routing.T, group_prob[None, :], expert_prob.T, tokens, cotangent,
        gate_weight, up_weight, down_weight,
    )
    tg, gg, ug, dg, gn, un, dn, epg, gpg = write_out(outs)
    return tg, gpg[0], epg.T, gg, ug, dg, gn, un, dn


def solution(mesh):
    return jax.shard_map(
        local,
        mesh=mesh,
        in_specs=(
            P("ep", None),
            P("ep", None),
            P("ep"),
            P("ep", None),
            P("ep", None),
            P("ep", None, "tp"),
            P("ep", None, "tp"),
            P("ep", "tp", None),
        ),
        out_specs=(
            P("ep", None),
            P("ep"),
            P("ep", None),
            P("ep", None, "tp"),
            P("ep", None, "tp"),
            P("ep", "tp", None),
            P("ep", None),
            P("ep", None),
            P("ep", "tp"),
        ),
        check_vma=False,
    )
```

```python
import functools
import jax
import jax.numpy as jnp
from jax import lax
from jax.experimental import pallas as pl
from jax.experimental.pallas import tpu as pltpu
from jax.sharding import PartitionSpec as P

MESH = pl.DeviceIdType.MESH
LANES = 128
F32 = jnp.float32
BF16 = jnp.bfloat16
CONTRACT_LAST = (((1,), (1,)), ((), ()))
SUM_PIECES = 4
GATHER_PIECES = 2
CHAIN_CORE = 1
STRIDE = 2
NEAR = ((0, 1), (0, 3), (1, 0), (3, 0), (1, 1), (1, 3), (3, 1), (3, 3))
FAR = (
    ((0, 2), (1, 2), (3, 2), (2, 2), (2, 0), (2, 1), (2, 3)),
    ((2, 0), (2, 1), (2, 3), (2, 2), (0, 2), (1, 2), (3, 2)),
)


def plane_peer(e, j, n_ep):
    if n_ep == 16:
        y, x = e // 4, e % 4
        return ((y + j // 4) % 4) * 4 + (x + j % 4) % 4
    return (e + j) % n_ep


def plane_source(e, j, n_ep):
    if n_ep == 16:
        y, x = e // 4, e % 4
        return ((y + 4 - j // 4) % 4) * 4 + (x + 4 - j % 4) % 4
    return (e + n_ep - j) % n_ep


def shifted(b, dy, dx):
    return ((b // 4 + dy + 4) % 4) * 4 + (b % 4 + dx + 4) % 4


def slot_rows(r, n_ep, cap):
    tok = r.shape[1]
    names = lax.broadcasted_iota(jnp.int32, (n_ep, tok), 0)
    first = (names == r[0:1, :]).astype(F32)
    second = (names == r[1:2, :]).astype(F32)
    earlier = lax.broadcasted_iota(jnp.int32, (tok, tok), 0) < lax.broadcasted_iota(
        jnp.int32, (tok, tok), 1
    )
    before = jnp.dot(
        (first + second).astype(BF16),
        jnp.where(earlier, 1.0, 0.0).astype(BF16),
        preferred_element_type=F32,
    )
    out = []
    for k, hot in enumerate((first, second)):
        place = jnp.sum(hot * before, axis=0, keepdims=True)
        out.append(r[k : k + 1, :].astype(F32) * float(cap) + place)
    return out


def body(
    n_ep, n_z, cap,
    r_ref, gp_ref, ep_ref, tok_hbm, cot_hbm, wg_hbm, wu_hbm, wd_hbm,
    tg_out, gg_out, ug_out, dg_out, gn_out, un_out, dn_out, epg_out, gpg_out,
    x, send, rows, wgu, wd, pre, hg, gpu, gput, hidt, prod,
    own, sib_send, sib_recv, dn_send, dn_recv, up_send, up_recv,
    sc_send, sc_recv, sm, sm_recv, sc_sib, sm_sib, sm_fin,
    fin, gat, tg, gg, ug, dg, dnacc,
    ld_sem, wl_sem, loc_sem, in_s, in_r, za_s, za_r, zb_s, zb_r, dx_s, dx_r, dy_s, dy_r,
    sc_s, sc_r, pt_s, pt_r, rd_s, rd_r, ru_s, ru_r, ms_s, ms_r, mx_s, mx_r, mg_s, mg_r,
    fa_s, fa_r, au_s, au_r, ad_s, ad_r, as_s, as_r, out_sem, met4, met8, pickt, hid,
):
    e, tp = lax.axis_index("ep"), lax.axis_index("tp")
    z, c = tp // 2, tp % 2
    par = z % 2
    mine, other = par * 2, 2 - par * 2
    near, far = z + 1 - 2 * par, (z + n_z - 1 + 2 * par) % n_z
    up_z, dn_z = (z + 1) % n_z, (z + n_z - 1) % n_z
    tok, quarter = x.shape[0], rows.shape[3]
    slots = n_ep * cap
    nd, nu = n_z // 2, n_z // 2 - 1
    qc = quarter // LANES
    sibling = (e, z * 2 + 1 - c)

    def at_z(other_z):
        return (e, other_z * 2 + c)

    def remote(src, dst, s_sem, r_sem, dev):
        return pltpu.make_async_remote_copy(
            src_ref=src, dst_ref=dst, send_sem=s_sem, recv_sem=r_sem,
            device_id=dev, device_id_type=MESH,
        )

    barrier = pltpu.get_barrier_semaphore()

    @pl.loop(1, n_ep)
    def _(j):
        pl.semaphore_signal(
            barrier, inc=1, device_id=(plane_peer(e, j, n_ep), tp), device_id_type=MESH
        )

    for step in (1, 2):
        for o in (z + step, z + n_z - step):
            pl.semaphore_signal(barrier, inc=1, device_id=at_z(o % n_z), device_id_type=MESH)
    pl.semaphore_signal(barrier, inc=1, device_id=sibling, device_id_type=MESH)

    def greet(sem, step):
        for o in (z + step, z + n_z - step):
            pl.semaphore_signal(sem, inc=1, device_id=at_z(o % n_z), device_id_type=MESH)

    start_col = pl.multiple_of(par * (2 * quarter), LANES)

    @pl.when(c == 0)
    def _():
        pltpu.make_async_copy(tok_hbm.at[:, pl.ds(start_col, 2 * quarter)], x, ld_sem).start()

    @pl.when(c == 1)
    def _():
        pltpu.make_async_copy(cot_hbm.at[:, pl.ds(start_col, 2 * quarter)], x, ld_sem).start()

    def weight_loads():
        out = []
        for q in range(4):
            span = pl.ds(q * quarter, quarter)
            out.append((wg_hbm.at[0, span, :], wgu.at[q, :, pl.ds(0, LANES)], wl_sem.at[q, 0]))
            out.append((wu_hbm.at[0, span, :], wgu.at[q, :, pl.ds(LANES, LANES)], wl_sem.at[q, 1]))
            out.append((wd_hbm.at[0, :, span], wd.at[q], wl_sem.at[q, 2]))
        return [pltpu.make_async_copy(*args) for args in out]

    for copy in weight_loads():
        copy.start()

    r = r_ref[...]
    weight = gp_ref[...] * ep_ref[...]
    w_eff = jnp.where(c == 0, jnp.ones_like(weight), weight)
    slot0, slot1 = slot_rows(r, n_ep, cap)
    pltpu.make_async_copy(tok_hbm.at[:, pl.ds(start_col, 2 * quarter)], x, ld_sem).wait()

    @pl.loop(0, slots // LANES)
    def _(i):
        at = pl.multiple_of(i * LANES, LANES)
        here = (lax.broadcasted_iota(jnp.int32, (LANES, tok), 0) + at).astype(F32)
        m0, m1 = here == slot0, here == slot1
        pick = jnp.where(m0 | m1, 1.0, 0.0).astype(BF16)
        scale = jnp.sum(
            jnp.where(m0, w_eff[0:1, :], 0.0) + jnp.where(m1, w_eff[1:2, :], 0.0),
            axis=1, keepdims=True,
        )
        got = scale * jnp.dot(pick, x[...], preferred_element_type=F32)
        send[0, pl.ds(at, LANES), :] = got[:, :quarter].astype(BF16)
        send[1, pl.ds(at, LANES), :] = got[:, quarter:].astype(BF16)

    pre[...] = jnp.zeros_like(pre)
    hg[...] = jnp.zeros_like(hg)
    pl.semaphore_wait(barrier, n_ep - 1 + 4 + 1)
    greet(met4, 2)

    def block(b):
        return pl.ds(pl.multiple_of(b * cap, 16), cap)

    def own_block():
        return pltpu.make_async_copy(
            send.at[:, block(e), :], rows.at[c, pl.ds(mine, 2), block(e), :], loc_sem.at[0]
        )

    def in_copy(src_block, to, sender):
        return remote(
            send.at[:, block(src_block), :], rows.at[c, pl.ds(mine, 2), block(sender), :],
            in_s.at[src_block], in_r.at[sender], (to, tp),
        )

    def za_copy(s, first):
        ref = rows.at[c, first, block(s), :]
        return remote(ref, ref, za_s.at[s], za_r.at[s], at_z(near))

    def zb_copy(s, first):
        ref = rows.at[c, first + 1, block(s), :]
        return remote(ref, ref, zb_s.at[s], zb_r.at[s], at_z(far))

    def dx_copy(s, arr):
        ref = rows.at[arr, pl.ds(mine, 2), block(s), :]
        return remote(ref, ref, dx_s.at[s], dx_r.at[s], sibling)

    def dy_copy(s, arr):
        ref = rows.at[arr, pl.ds(other, 2), block(s), :]
        return remote(ref, ref, dy_s.at[s], dy_r.at[s], sibling)

    def pass_on(s):
        za_copy(s, mine).start()
        zb_copy(s, mine).start()
        dx_copy(s, c).start()

    def exchange(order):
        for dy, dx in order:
            p = shifted(e, dy, dx) if n_ep == 16 else (e + dx) % n_ep
            in_copy(p, p, e).start()
        own_block().wait()
        pass_on(e)
        for dy, dx in order:
            s = shifted(e, -dy, -dx) if n_ep == 16 else (e - dx + n_ep) % n_ep
            in_copy(s, s, s).wait_recv()
            pass_on(s)

    own_block().start()
    for core in range(2):
        @pl.when(c == core)
        def _():
            exchange(NEAR + FAR[core] if n_ep == 16 else [(0, j) for j in range(1, n_ep)])

    def gate_up_part(q):
        pre[...] += jnp.dot(rows[0, q], wgu[q], preferred_element_type=F32)

    def down_part(q):
        hg[...] += lax.dot_general(rows[1, q], wd[q], CONTRACT_LAST, preferred_element_type=F32)

    def multiply(first, arr_is_own):
        is_in = (c == 0) if arr_is_own else (c == 1)

        @pl.when(is_in)
        def _():
            @pl.loop(0, 2)
            def _(i):
                gate_up_part(first + i)

        @pl.when(jnp.logical_not(is_in))
        def _():
            @pl.loop(0, 2)
            def _(i):
                down_part(first + i)

    for copy in weight_loads():
        copy.wait()
    pl.semaphore_wait(met4, 2)
    greet(met8, 4)
    multiply(mine, True)

    @pl.loop(0, n_ep)
    def _(j):
        s = plane_source(e, j, n_ep)
        za_copy(s, other).wait_recv()
        zb_copy(s, other).wait_recv()
        dy_copy(s, c).start()

    multiply(other, True)

    @pl.loop(0, n_ep)
    def _(j):
        dx_copy(plane_source(e, j, n_ep), 1 - c).wait_recv()

    multiply(mine, False)

    @pl.loop(0, n_ep)
    def _(j):
        dy_copy(plane_source(e, j, n_ep), 1 - c).wait_recv()

    pl.semaphore_wait(met8, 2)
    multiply(other, False)

    @pl.loop(0, slots // LANES)
    def _(i):
        at = pl.ds(pl.multiple_of(i * LANES, LANES), LANES)
        gate, upv, grad = pre[at, :LANES], pre[at, LANES:], hg[at, :]
        sigma = jax.nn.sigmoid(gate)
        activated = gate * sigma
        derivative = sigma * (1.0 + gate * (1.0 - sigma))
        hidden = (activated * upv).astype(BF16)
        prod[at, :] = hidden.astype(F32) * grad
        hid[at, :] = hidden
        gpu[at, :LANES] = (grad * upv * derivative).astype(BF16)
        gpu[at, LANES:] = (grad * activated).astype(BF16)

    def sc_copy(to, sender):
        return remote(sc_send.at[to], sc_recv.at[sender], sc_s.at[to], sc_r.at[sender], (to, tp))

    def pt_copy(o):
        return remote(sib_send.at[o], sib_recv.at[o], pt_s.at[o], pt_r.at[o], sibling)

    def input_part(q):
        return lax.dot_general(gpu[...], wgu[q], CONTRACT_LAST, preferred_element_type=F32)

    def quarters():
        return [((z + nd) // qc + step) % 4 for step in (0, 3, 1, 2)]

    @pl.when(c != CHAIN_CORE)
    def _():
        for q in quarters():
            part = input_part(q)
            for i in range(qc):
                sib_send[q * qc + i] = part[:, i * LANES : (i + 1) * LANES].astype(BF16)
                pt_copy(q * qc + i).start()

    @pl.when(c == CHAIN_CORE)
    def _():
        for q in quarters():
            part = input_part(q)
            for i in range(qc):
                own[q * qc + i] = part[:, i * LANES : (i + 1) * LANES]

    dnacc[...] = jnp.zeros_like(dnacc)

    def turn_piece(source, target):
        @pl.loop(0, slots // LANES)
        def _(i):
            at = pl.ds(pl.multiple_of(i * LANES, LANES), LANES)
            target[:, at] = source[at, :].astype(F32).T.astype(BF16)

    def down_piece(q):
        down = jnp.dot(hidt[...], rows[1, q], preferred_element_type=F32)
        dg[:, q * quarter : (q + 1) * quarter] = down.astype(BF16)
        square = down * down
        dnacc[...] += sum(square[:, i * LANES : (i + 1) * LANES] for i in range(qc))

    def in_piece(k, q):
        target = (gg, ug)[k]
        both = jnp.dot(gput[k * LANES : (k + 1) * LANES, :], rows[0, q], preferred_element_type=F32)
        norm = jnp.sum(both * both, axis=0, keepdims=True)
        for i in range(qc):
            sm[q * qc + i, :, k * LANES : (k + 1) * LANES] = norm[:, i * LANES : (i + 1) * LANES]
        target[q * quarter : (q + 1) * quarter, :] = both.T.astype(BF16)

    def pick_piece():
        lane = lax.broadcasted_iota(jnp.int32, (slots, tok), 0).astype(F32)
        pick = jnp.where((lane == slot0) | (lane == slot1), 1.0, 0.0)
        pickt[...] = pick.T.astype(BF16)

    def grad_stores():
        return [
            pltpu.make_async_copy(gg, gg_out.at[0], out_sem.at[0]),
            pltpu.make_async_copy(ug, ug_out.at[0], out_sem.at[1]),
            pltpu.make_async_copy(dg, dg_out.at[0], out_sem.at[2]),
        ]

    def own_scores():
        sc_recv[e] = sc_send[e]

    def ms_copy(o, sender):
        return remote(sm.at[o], sm_recv.at[sender], ms_s.at[o], ms_r.at[sender], at_z(o))

    def hand_copy(i):
        src, dst = ((sc_send, sc_sib), (sm, sm_sib), (sm_fin, sm_fin))[i]
        return remote(src, dst, mx_s.at[i], mx_r.at[i], sibling)

    def mg_copy(piece, to):
        return remote(sm_fin.at[piece], sm_fin.at[piece], mg_s.at[to], mg_r.at[piece], at_z(to))

    score_rows = tok // LANES

    def clear_scores():
        sm[:, :, 2 * LANES :] = jnp.zeros((n_z, 1, LANES), F32)

    def small_start():
        own_scores()

        @pl.loop(1, n_ep)
        def _(j):
            s = plane_source(e, j, n_ep)
            sc_copy(s, s).wait_recv()

        got = sc_recv[...].reshape(n_ep, sc_recv.shape[2])
        fill = jnp.zeros((LANES - n_ep, got.shape[1]), F32)
        columns = jnp.concatenate([got, fill], axis=0).T
        totals = [jnp.zeros((1, tok), F32), jnp.zeros((1, tok), F32)]
        lane = lax.broadcasted_iota(jnp.int32, (cap, tok), 0)
        for s in range(n_ep):
            here = (lane + s * cap).astype(F32)
            column = columns[:cap, s : s + 1]
            for k, slot in enumerate((slot0, slot1)):
                totals[k] += jnp.sum(jnp.where(here == slot, column, 0.0), axis=0, keepdims=True)
        clear_scores()
        for k in range(2):
            for h in range(score_rows):
                sm[k * score_rows + h, :, 2 * LANES :] = totals[k][:, h * LANES : (h + 1) * LANES]

        hand_copy(1).wait_recv()
        sm[...] += sm_sib[...]

        @pl.loop(1, n_z)
        def _(j):
            o = (z + j) % n_z
            ms_copy(o, z).start()

    def small_middle():
        @pl.loop(1, n_z)
        def _(j):
            s = (z + j) % n_z
            ms_copy(s, s).wait_recv()

        sm_recv[z] = sm[z]
        sm_fin[z] = jnp.sum(sm_recv[...], axis=0)

        @pl.loop(1, n_z)
        def _(j):
            mg_copy(z, (z + j) % n_z).start()

    def small_end():
        @pl.loop(1, n_z)
        def _(j):
            o = (z + j) % n_z
            mg_copy(o, o).wait_recv()

        hand_copy(2).start()

    def scores():
        ones = jnp.ones((8, LANES), F32)
        for b in range(n_ep):
            row = lax.dot_general(
                ones, prod[b * cap : (b + 1) * cap, :], CONTRACT_LAST,
                precision=lax.Precision.HIGHEST, preferred_element_type=F32,
            )
            sc_send[b, :, :cap] = row[0:1, :]

    def scores_send():
        hand_copy(0).wait_recv()
        sc_send[...] += sc_sib[...]

        @pl.loop(1, n_ep)
        def _(j):
            p = plane_peer(e, j, n_ep)
            sc_copy(p, e).start()

    def store_start():
        for copy in grad_stores():
            copy.start()

    work = []
    work += [functools.partial(turn_piece, hid, hidt), functools.partial(turn_piece, gpu, gput)]
    for q in range(4):
        work += [functools.partial(down_piece, q)]
        work += [functools.partial(in_piece, 0, q), functools.partial(in_piece, 1, q)]
    work += [store_start]

    sub = slots // SUM_PIECES

    def part(h):
        return pl.ds(h * sub, sub)

    def rd_copy(t, h):
        return remote(
            dn_send.at[t, part(h), :], dn_recv.at[t, part(h), :],
            rd_s.at[t, h], rd_r.at[t, h], at_z(dn_z),
        )

    def ru_copy(t, h):
        return remote(
            up_send.at[t, part(h), :], up_recv.at[t, part(h), :],
            ru_s.at[t, h], ru_r.at[t, h], at_z(up_z),
        )

    def chip_sum(o, h):
        return own[o, part(h), :] + sib_recv[o, part(h), :].astype(F32)

    @pl.when(c != CHAIN_CORE)
    def _():
        for step in [scores, scores_send] + work + [small_start, small_middle, small_end]:
            step()

    @pl.when(c == CHAIN_CORE)
    def _():
        todo = [scores, hand_copy(0).start] + work + [clear_scores, hand_copy(1).start, pick_piece]
        for t in range(nd):
            o_dn, o_up = (z + n_z - nd + t) % n_z, (z + nu - t + n_z) % n_z
            pt_copy(o_dn).wait_recv()
            pt_copy(o_up).wait_recv()
            for h in range(SUM_PIECES):
                total = chip_sum(o_dn, h)
                if t > 0:
                    rd_copy(t - 1, h).wait_recv()
                    total += dn_recv[t - 1, part(h), :].astype(F32)
                dn_send[t, part(h), :] = total.astype(BF16)
                rd_copy(t, h).start()
                if t < nu:
                    total = chip_sum(o_up, h)
                    if t > 0:
                        ru_copy(t - 1, h).wait_recv()
                        total += up_recv[t - 1, part(h), :].astype(F32)
                    up_send[t, part(h), :] = total.astype(BF16)
                    ru_copy(t, h).start()
                for _ in range(min(t, 1) if n_z == 16 else len(todo)):
                    if todo:
                        todo.pop(0)()

        for h in range(SUM_PIECES):
            total = chip_sum(z, h)
            ru_copy(nu - 1, h).wait_recv()
            total += up_recv[nu - 1, part(h), :].astype(F32)
            rd_copy(nd - 1, h).wait_recv()
            total += dn_recv[nd - 1, part(h), :].astype(F32)
            fin[part(h), :] = total.astype(BF16)

    def fa_copy(b, sender):
        return remote(
            fin.at[block(b), :], gat.at[block(sender), :], fa_s.at[b], fa_r.at[sender], (b, tp)
        )

    def fa_local():
        return pltpu.make_async_copy(fin.at[block(e), :], gat.at[block(e), :], loc_sem.at[1])

    piece = tok // GATHER_PIECES

    def chunk(o, h):
        return tg.at[pl.ds(h * piece, piece), pl.ds(pl.multiple_of(o * LANES, LANES), LANES)]

    def au_copy(t, h, o):
        ref = chunk(o, h)
        hop = 1 if t == 1 else STRIDE
        return remote(ref, ref, au_s.at[t, h], au_r.at[t, h], at_z((z + hop) % n_z))

    def ad_copy(t, h, o):
        ref = chunk(o, h)
        hop = 1 if t == 1 else STRIDE
        return remote(ref, ref, ad_s.at[t, h], ad_r.at[t, h], at_z((z + n_z - hop) % n_z))

    def as_copy(o, h):
        ref = chunk(o, h)
        return remote(ref, ref, as_s.at[o, h], as_r.at[o, h], sibling)

    def store(o):
        at = pl.ds(pl.multiple_of(o * LANES, LANES), LANES)
        return pltpu.make_async_copy(tg.at[:, at], tg_out.at[:, at], out_sem.at[3])

    @pl.when(c == CHAIN_CORE)
    def _():
        fa_local().start()

        @pl.loop(1, n_ep)
        def _(j):
            fa_copy(plane_peer(e, j, n_ep), e).start()

        fa_local().wait()

        @pl.loop(1, n_ep)
        def _(j):
            s = plane_source(e, j, n_ep)
            fa_copy(s, s).wait_recv()

        for h in range(GATHER_PIECES):
            at = slice(h * piece, (h + 1) * piece)
            acc = jnp.dot(pickt[at, :], gat[...], preferred_element_type=F32)
            tg[at, pl.ds(pl.multiple_of(z * LANES, LANES), LANES)] = acc.astype(BF16)
            for t in range(1, STRIDE + 1):
                if t <= nu:
                    au_copy(t, h, z).start()
                ad_copy(t, h, z).start()
            as_copy(z, h).start()
        store(z).start()
        for t in range(1, nd + 1):
            for h in range(GATHER_PIECES):
                if t <= nu:
                    o = (z + n_z - t) % n_z
                    au_copy(t, h, o).wait_recv()
                    if t + STRIDE <= nu:
                        au_copy(t + STRIDE, h, o).start()
                    as_copy(o, h).start()
                o = (z + t) % n_z
                ad_copy(t, h, o).wait_recv()
                if t + STRIDE <= nd:
                    ad_copy(t + STRIDE, h, o).start()
                as_copy(o, h).start()
            if t <= nu:
                store((z + n_z - t) % n_z).start()
            store((z + t) % n_z).start()

    @pl.when(c == CHAIN_CORE)
    def _():
        hand_copy(2).wait_recv()

    units = float(LANES * 2 * n_z)
    for o in range(n_z):
        gn_out[:, o * LANES : (o + 1) * LANES] = sm_fin[o, :, :LANES] / units
        un_out[:, o * LANES : (o + 1) * LANES] = sm_fin[o, :, LANES : 2 * LANES] / units
    dn_out[...] = lax.dot_general(
        jnp.ones((8, LANES), F32), dnacc[...], CONTRACT_LAST,
        precision=lax.Precision.HIGHEST, preferred_element_type=F32,
    )[0:1, :] / float(LANES * n_z)
    for h in range(score_rows):
        at = slice(h * LANES, (h + 1) * LANES)
        gp = gp_ref[:, at]
        total = jnp.zeros((1, LANES), F32)
        for k in range(2):
            ep = ep_ref[k : k + 1, at]
            score = sm_fin[k * score_rows + h, :, 2 * LANES :] / (gp * ep)
            epg_out[k : k + 1, at] = gp * score
            total += ep * score
        gpg_out[:, at] = total

    @pl.when(c != CHAIN_CORE)
    def _():
        @pl.loop(0, n_z)
        def _(j):
            o = (z + n_z + (j % 2) * j - j // 2) % n_z
            for h in range(GATHER_PIECES):
                as_copy(o, h).wait_recv()
            store(o).start()

    for copy in grad_stores():
        copy.wait()

    @pl.loop(1, n_ep)
    def _(j):
        p = plane_peer(e, j, n_ep)
        in_copy(p, p, e).wait_send()

    @pl.loop(0, n_ep)
    def _(s):
        za_copy(s, mine).wait_send()
        zb_copy(s, mine).wait_send()
        dx_copy(s, c).wait_send()
        dy_copy(s, c).wait_send()

    @pl.when(c != CHAIN_CORE)
    def _():
        @pl.loop(1, n_ep)
        def _(j):
            sc_copy(plane_peer(e, j, n_ep), e).wait_send()

        @pl.loop(1, n_z)
        def _(j):
            o = (z + j) % n_z
            ms_copy(o, z).wait_send()
            mg_copy(z, o).wait_send()

        hand_copy(2).wait_send()

        @pl.loop(0, n_z)
        def _(o):
            pt_copy(o).wait_send()

    @pl.when(c == CHAIN_CORE)
    def _():
        hand_copy(0).wait_send()
        hand_copy(1).wait_send()

        @pl.loop(1, n_ep)
        def _(j):
            fa_copy(plane_peer(e, j, n_ep), e).wait_send()

        for h in range(SUM_PIECES):
            for t in range(nd):
                rd_copy(t, h).wait_send()
            for t in range(nu):
                ru_copy(t, h).wait_send()

    @pl.when(c == CHAIN_CORE)
    def _():
        for h in range(GATHER_PIECES):
            for t in range(1, nu + 1):
                au_copy(t, h, z).wait_send()
            for t in range(1, nd + 1):
                ad_copy(t, h, z).wait_send()

            @pl.loop(0, n_z)
            def _(o):
                as_copy(o, h).wait_send()

    pltpu.make_async_copy(tg, tg_out, out_sem.at[3]).wait()


def flush(count, *refs):
    ins, outs, bufs = refs[:count], refs[count : 2 * count], refs[2 * count : 3 * count]
    in_sem, out_sem = refs[3 * count :]
    reads, writes = [], []
    for i in range(count):
        rows = ins[i].shape[-2]
        pieces = 4 if rows % 64 == 0 else 1
        for p in range(pieces):
            at = pl.ds(p * (rows // pieces), rows // pieces)
            src, buf, dst = (
                (ref.at[at, :] if len(ref.shape) == 2 else ref.at[:, at, :])
                for ref in (ins[i], bufs[i], outs[i])
            )
            reads.append(pltpu.make_async_copy(src, buf, in_sem.at[i, p]))
            writes.append(pltpu.make_async_copy(buf, dst, out_sem.at[i, p]))
    for copy in reads:
        copy.start()
    for read, write in zip(reads, writes):
        read.wait()
        write.start()
    for copy in writes:
        copy.wait()


def write_out(arrays):
    count = len(arrays)
    any_spec = pl.BlockSpec(memory_space=pl.ANY)
    return pl.pallas_call(
        functools.partial(flush, count),
        out_shape=tuple(jax.ShapeDtypeStruct(a.shape, a.dtype) for a in arrays),
        in_specs=[any_spec] * count,
        out_specs=(any_spec,) * count,
        scratch_shapes=[pltpu.VMEM(a.shape, a.dtype) for a in arrays]
        + [pltpu.SemaphoreType.DMA((count, 4)), pltpu.SemaphoreType.DMA((count, 4))],
    )(*arrays)


def local(tokens, cotangent, group_prob, expert_prob, routing, gate_weight, up_weight, down_weight):
    tok, width = tokens.shape
    n_ep = lax.axis_size("ep")
    n_z = lax.axis_size("tp") // 2
    cap = 3 * tok * 2 // (2 * n_ep)
    slots = n_ep * cap
    quarter = width // 4
    unit = gate_weight.shape[2]
    nd, nu = n_z // 2, n_z // 2 - 1
    scw = -(-cap // LANES) * LANES
    dma = pltpu.SemaphoreType.DMA
    vm = pltpu.VMEM
    any_spec = pl.BlockSpec(memory_space=pl.ANY)
    vm_spec = pl.BlockSpec(memory_space=pltpu.VMEM)
    outs = pl.pallas_call(
        functools.partial(body, n_ep, n_z, cap),
        out_shape=(
            jax.ShapeDtypeStruct((tok, width), BF16),
            jax.ShapeDtypeStruct((1, width, unit), BF16),
            jax.ShapeDtypeStruct((1, width, unit), BF16),
            jax.ShapeDtypeStruct((1, unit, width), BF16),
            jax.ShapeDtypeStruct((1, width), F32),
            jax.ShapeDtypeStruct((1, width), F32),
            jax.ShapeDtypeStruct((1, unit), F32),
            jax.ShapeDtypeStruct((2, tok), F32),
            jax.ShapeDtypeStruct((1, tok), F32),
        ),
        in_specs=[vm_spec] * 3 + [any_spec] * 5,
        out_specs=(any_spec,) * 4 + (vm_spec,) * 5,
        scratch_shapes=[
            vm((tok, 2 * quarter), BF16),
            vm((2, slots, quarter), BF16),
            vm((2, 4, slots, quarter), BF16),
            vm((4, quarter, 2 * unit), BF16),
            vm((4, unit, quarter), BF16),
            vm((slots, 2 * unit), F32),
            vm((slots, unit), F32),
            vm((slots, 2 * unit), BF16),
            vm((2 * unit, slots), BF16),
            vm((unit, slots), BF16),
            vm((slots, unit), F32),
            vm((n_z, slots, LANES), F32),
            vm((n_z, slots, LANES), BF16),
            vm((n_z, slots, LANES), BF16),
            vm((nd, slots, LANES), BF16),
            vm((nd, slots, LANES), BF16),
            vm((nu, slots, LANES), BF16),
            vm((nu, slots, LANES), BF16),
            vm((n_ep, 1, scw), F32),
            vm((n_ep, 1, scw), F32),
            vm((n_z, 1, 3 * LANES), F32),
            vm((n_z, 1, 3 * LANES), F32),
            vm((n_ep, 1, scw), F32),
            vm((n_z, 1, 3 * LANES), F32),
            vm((n_z, 1, 3 * LANES), F32),
            vm((slots, LANES), BF16),
            vm((slots, LANES), BF16),
            vm((tok, width), BF16),
            vm((width, unit), BF16),
            vm((width, unit), BF16),
            vm((unit, width), BF16),
            vm((unit, LANES), F32),
            dma, dma((4, 3)), dma((2,)),
            dma((n_ep,)), dma((n_ep,)), dma((n_ep,)), dma((n_ep,)), dma((n_ep,)), dma((n_ep,)),
            dma((n_ep,)), dma((n_ep,)), dma((n_ep,)), dma((n_ep,)),
            dma((n_ep,)), dma((n_ep,)),
            dma((n_z,)), dma((n_z,)),
            dma((nd, SUM_PIECES)), dma((nd, SUM_PIECES)), dma((nu, SUM_PIECES)), dma((nu, SUM_PIECES)),
            dma((n_z,)), dma((n_z,)), dma((3,)), dma((3,)), dma((n_z,)), dma((n_z,)),
            dma((n_ep,)), dma((n_ep,)),
            dma((nu + 1, GATHER_PIECES)), dma((nu + 1, GATHER_PIECES)),
            dma((nd + 1, GATHER_PIECES)), dma((nd + 1, GATHER_PIECES)),
            dma((n_z, GATHER_PIECES)), dma((n_z, GATHER_PIECES)),
            dma((4,)), pltpu.SemaphoreType.REGULAR, pltpu.SemaphoreType.REGULAR,
            vm((tok, slots), BF16),
            vm((slots, unit), BF16),
        ],
        compiler_params=pltpu.CompilerParams(
            collective_id=0, has_side_effects=True, vmem_limit_bytes=56 * 1024 * 1024
        ),
    )(
        routing.T, group_prob[None, :], expert_prob.T, tokens, cotangent,
        gate_weight, up_weight, down_weight,
    )
    tg, gg, ug, dg, gn, un, dn, epg, gpg = write_out(outs)
    return tg, gpg[0], epg.T, gg, ug, dg, gn, un, dn


def solution(mesh):
    return jax.shard_map(
        local,
        mesh=mesh,
        in_specs=(
            P("ep", None),
            P("ep", None),
            P("ep"),
            P("ep", None),
            P("ep", None),
            P("ep", None, "tp"),
            P("ep", None, "tp"),
            P("ep", "tp", None),
        ),
        out_specs=(
            P("ep", None),
            P("ep"),
            P("ep", None),
            P("ep", None, "tp"),
            P("ep", None, "tp"),
            P("ep", "tp", None),
            P("ep", None),
            P("ep", None),
            P("ep", "tp"),
        ),
        check_vma=False,
    )
```

```python
import functools
import jax
import jax.numpy as jnp
from jax import lax
from jax.experimental import pallas as pl
from jax.experimental.pallas import tpu as pltpu
from jax.sharding import PartitionSpec as P

MESH = pl.DeviceIdType.MESH
LANES = 128
F32 = jnp.float32
BF16 = jnp.bfloat16
CONTRACT_LAST = (((1,), (1,)), ((), ()))
SUM_PIECES = 4
GATHER_PIECES = 2
CHAIN_CORE = 1
STRIDE = 2
NEAR = ((0, 1), (0, 3), (1, 0), (3, 0), (1, 1), (1, 3), (3, 1), (3, 3))
FAR = (
    ((0, 2), (1, 2), (3, 2), (2, 2), (2, 0), (2, 1), (2, 3)),
    ((2, 0), (2, 1), (2, 3), (2, 2), (0, 2), (1, 2), (3, 2)),
)


def plane_peer(e, j, n_ep):
    if n_ep == 16:
        y, x = e // 4, e % 4
        return ((y + j // 4) % 4) * 4 + (x + j % 4) % 4
    return (e + j) % n_ep


def plane_source(e, j, n_ep):
    if n_ep == 16:
        y, x = e // 4, e % 4
        return ((y + 4 - j // 4) % 4) * 4 + (x + 4 - j % 4) % 4
    return (e + n_ep - j) % n_ep


def shifted(b, dy, dx):
    return ((b // 4 + dy + 4) % 4) * 4 + (b % 4 + dx + 4) % 4


def slot_rows(r, n_ep, cap):
    tok = r.shape[1]
    names = lax.broadcasted_iota(jnp.int32, (n_ep, tok), 0)
    first = (names == r[0:1, :]).astype(F32)
    second = (names == r[1:2, :]).astype(F32)
    earlier = lax.broadcasted_iota(jnp.int32, (tok, tok), 0) < lax.broadcasted_iota(
        jnp.int32, (tok, tok), 1
    )
    before = jnp.dot(
        (first + second).astype(BF16),
        jnp.where(earlier, 1.0, 0.0).astype(BF16),
        preferred_element_type=F32,
    )
    out = []
    for k, hot in enumerate((first, second)):
        place = jnp.sum(hot * before, axis=0, keepdims=True)
        out.append(r[k : k + 1, :].astype(F32) * float(cap) + place)
    return out


def body(
    n_ep, n_z, cap,
    r_ref, gp_ref, ep_ref, tok_hbm, cot_hbm, wg_hbm, wu_hbm, wd_hbm,
    tg_out, gg_out, ug_out, dg_out, gn_out, un_out, dn_out, epg_out, gpg_out,
    x, send, rows, wgu, wd, pre, hg, gpu, gput, hidt, prod,
    own, sib_send, sib_recv, dn_send, dn_recv, up_send, up_recv,
    sc_send, sc_recv, sm, sm_recv, sc_sib, sm_sib, sm_fin,
    fin, gat, tg, gg, ug, dg, dnacc,
    ld_sem, wl_sem, loc_sem, in_s, in_r, za_s, za_r, zb_s, zb_r, dx_s, dx_r, dy_s, dy_r,
    sc_s, sc_r, pt_s, pt_r, rd_s, rd_r, ru_s, ru_r, ms_s, ms_r, mx_s, mx_r, mg_s, mg_r,
    fa_s, fa_r, au_s, au_r, ad_s, ad_r, as_s, as_r, out_sem, met4, met8, pickt, hid,
):
    e, tp = lax.axis_index("ep"), lax.axis_index("tp")
    z, c = tp // 2, tp % 2
    par = z % 2
    mine, other = par * 2, 2 - par * 2
    near, far = z + 1 - 2 * par, (z + n_z - 1 + 2 * par) % n_z
    up_z, dn_z = (z + 1) % n_z, (z + n_z - 1) % n_z
    tok, quarter = x.shape[0], rows.shape[3]
    slots = n_ep * cap
    nd, nu = n_z // 2, n_z // 2 - 1
    qc = quarter // LANES
    sibling = (e, z * 2 + 1 - c)

    def at_z(other_z):
        return (e, other_z * 2 + c)

    def remote(src, dst, s_sem, r_sem, dev):
        return pltpu.make_async_remote_copy(
            src_ref=src, dst_ref=dst, send_sem=s_sem, recv_sem=r_sem,
            device_id=dev, device_id_type=MESH,
        )

    barrier = pltpu.get_barrier_semaphore()

    @pl.loop(1, n_ep)
    def _(j):
        pl.semaphore_signal(
            barrier, inc=1, device_id=(plane_peer(e, j, n_ep), tp), device_id_type=MESH
        )

    for step in (1, 2):
        for o in (z + step, z + n_z - step):
            pl.semaphore_signal(barrier, inc=1, device_id=at_z(o % n_z), device_id_type=MESH)
    pl.semaphore_signal(barrier, inc=1, device_id=sibling, device_id_type=MESH)

    def greet(sem, step):
        for o in (z + step, z + n_z - step):
            pl.semaphore_signal(sem, inc=1, device_id=at_z(o % n_z), device_id_type=MESH)

    start_col = pl.multiple_of(par * (2 * quarter), LANES)

    @pl.when(c == 0)
    def _():
        pltpu.make_async_copy(tok_hbm.at[:, pl.ds(start_col, 2 * quarter)], x, ld_sem).start()

    @pl.when(c == 1)
    def _():
        pltpu.make_async_copy(cot_hbm.at[:, pl.ds(start_col, 2 * quarter)], x, ld_sem).start()

    def weight_loads():
        out = []
        for q in range(4):
            span = pl.ds(q * quarter, quarter)
            out.append((wg_hbm.at[0, span, :], wgu.at[q, :, pl.ds(0, LANES)], wl_sem.at[q, 0]))
            out.append((wu_hbm.at[0, span, :], wgu.at[q, :, pl.ds(LANES, LANES)], wl_sem.at[q, 1]))
            out.append((wd_hbm.at[0, :, span], wd.at[q], wl_sem.at[q, 2]))
        return [pltpu.make_async_copy(*args) for args in out]

    for copy in weight_loads():
        copy.start()

    r = r_ref[...]
    weight = gp_ref[...] * ep_ref[...]
    w_eff = jnp.where(c == 0, jnp.ones_like(weight), weight)
    slot0, slot1 = slot_rows(r, n_ep, cap)
    pltpu.make_async_copy(tok_hbm.at[:, pl.ds(start_col, 2 * quarter)], x, ld_sem).wait()

    @pl.loop(0, slots // LANES)
    def _(i):
        at = pl.multiple_of(i * LANES, LANES)
        here = (lax.broadcasted_iota(jnp.int32, (LANES, tok), 0) + at).astype(F32)
        m0, m1 = here == slot0, here == slot1
        pick = jnp.where(m0 | m1, 1.0, 0.0).astype(BF16)
        scale = jnp.sum(
            jnp.where(m0, w_eff[0:1, :], 0.0) + jnp.where(m1, w_eff[1:2, :], 0.0),
            axis=1, keepdims=True,
        )
        got = scale * jnp.dot(pick, x[...], preferred_element_type=F32)
        send[0, pl.ds(at, LANES), :] = got[:, :quarter].astype(BF16)
        send[1, pl.ds(at, LANES), :] = got[:, quarter:].astype(BF16)

    pre[...] = jnp.zeros_like(pre)
    hg[...] = jnp.zeros_like(hg)
    pl.semaphore_wait(barrier, n_ep - 1 + 4 + 1)
    greet(met4, 2)

    def block(b):
        return pl.ds(pl.multiple_of(b * cap, 16), cap)

    def own_block():
        return pltpu.make_async_copy(
            send.at[:, block(e), :], rows.at[c, pl.ds(mine, 2), block(e), :], loc_sem.at[0]
        )

    def in_copy(src_block, to, sender):
        return remote(
            send.at[:, block(src_block), :], rows.at[c, pl.ds(mine, 2), block(sender), :],
            in_s.at[src_block], in_r.at[sender], (to, tp),
        )

    def za_copy(s, first):
        ref = rows.at[c, first, block(s), :]
        return remote(ref, ref, za_s.at[s], za_r.at[s], at_z(near))

    def zb_copy(s, first):
        ref = rows.at[c, first + 1, block(s), :]
        return remote(ref, ref, zb_s.at[s], zb_r.at[s], at_z(far))

    def dx_copy(s, arr):
        ref = rows.at[arr, pl.ds(mine, 2), block(s), :]
        return remote(ref, ref, dx_s.at[s], dx_r.at[s], sibling)

    def dy_copy(s, arr):
        ref = rows.at[arr, pl.ds(other, 2), block(s), :]
        return remote(ref, ref, dy_s.at[s], dy_r.at[s], sibling)

    def pass_on(s):
        za_copy(s, mine).start()
        zb_copy(s, mine).start()
        dx_copy(s, c).start()

    def exchange(order):
        for dy, dx in order:
            p = shifted(e, dy, dx) if n_ep == 16 else (e + dx) % n_ep
            in_copy(p, p, e).start()
        own_block().wait()
        pass_on(e)
        for dy, dx in order:
            s = shifted(e, -dy, -dx) if n_ep == 16 else (e - dx + n_ep) % n_ep
            in_copy(s, s, s).wait_recv()
            pass_on(s)

    own_block().start()
    for core in range(2):
        @pl.when(c == core)
        def _():
            exchange(NEAR + FAR[core] if n_ep == 16 else [(0, j) for j in range(1, n_ep)])

    def gate_up_part(q):
        pre[...] += jnp.dot(rows[0, q], wgu[q], preferred_element_type=F32)

    def down_part(q):
        hg[...] += lax.dot_general(rows[1, q], wd[q], CONTRACT_LAST, preferred_element_type=F32)

    def multiply(first, arr_is_own):
        is_in = (c == 0) if arr_is_own else (c == 1)

        @pl.when(is_in)
        def _():
            @pl.loop(0, 2)
            def _(i):
                gate_up_part(first + i)

        @pl.when(jnp.logical_not(is_in))
        def _():
            @pl.loop(0, 2)
            def _(i):
                down_part(first + i)

    for copy in weight_loads():
        copy.wait()
    pl.semaphore_wait(met4, 2)
    greet(met8, 4)
    multiply(mine, True)

    @pl.loop(0, n_ep)
    def _(j):
        s = plane_source(e, j, n_ep)
        za_copy(s, other).wait_recv()
        zb_copy(s, other).wait_recv()
        dy_copy(s, c).start()

    multiply(other, True)

    @pl.loop(0, n_ep)
    def _(j):
        dx_copy(plane_source(e, j, n_ep), 1 - c).wait_recv()

    multiply(mine, False)

    @pl.loop(0, n_ep)
    def _(j):
        dy_copy(plane_source(e, j, n_ep), 1 - c).wait_recv()

    pl.semaphore_wait(met8, 2)
    multiply(other, False)

    @pl.loop(0, slots // LANES)
    def _(i):
        at = pl.ds(pl.multiple_of(i * LANES, LANES), LANES)
        gate, upv, grad = pre[at, :LANES], pre[at, LANES:], hg[at, :]
        sigma = jax.nn.sigmoid(gate)
        activated = gate * sigma
        derivative = sigma * (1.0 + gate * (1.0 - sigma))
        hidden = (activated * upv).astype(BF16)
        prod[at, :] = hidden.astype(F32) * grad
        hid[at, :] = hidden
        gpu[at, :LANES] = (grad * upv * derivative).astype(BF16)
        gpu[at, LANES:] = (grad * activated).astype(BF16)

    def sc_copy(to, sender):
        return remote(sc_send.at[to], sc_recv.at[sender], sc_s.at[to], sc_r.at[sender], (to, tp))

    def pt_copy(o):
        return remote(sib_send.at[o], sib_recv.at[o], pt_s.at[o], pt_r.at[o], sibling)

    def input_part(q):
        return lax.dot_general(gpu[...], wgu[q], CONTRACT_LAST, preferred_element_type=F32)

    def quarters():
        return [((z + nd) // qc + step) % 4 for step in (0, 3, 1, 2)]

    @pl.when(c != CHAIN_CORE)
    def _():
        for q in quarters():
            part = input_part(q)
            for i in range(qc):
                sib_send[q * qc + i] = part[:, i * LANES : (i + 1) * LANES].astype(BF16)
                pt_copy(q * qc + i).start()

    @pl.when(c == CHAIN_CORE)
    def _():
        for q in quarters():
            part = input_part(q)
            for i in range(qc):
                own[q * qc + i] = part[:, i * LANES : (i + 1) * LANES]

    dnacc[...] = jnp.zeros_like(dnacc)

    def turn_piece(source, target):
        @pl.loop(0, slots // LANES)
        def _(i):
            at = pl.ds(pl.multiple_of(i * LANES, LANES), LANES)
            target[:, at] = source[at, :].astype(F32).T.astype(BF16)

    def down_piece(q):
        down = jnp.dot(hidt[...], rows[1, q], preferred_element_type=F32)
        dg[:, q * quarter : (q + 1) * quarter] = down.astype(BF16)
        square = down * down
        dnacc[...] += sum(square[:, i * LANES : (i + 1) * LANES] for i in range(qc))

    def in_piece(k, q):
        target = (gg, ug)[k]
        both = jnp.dot(gput[k * LANES : (k + 1) * LANES, :], rows[0, q], preferred_element_type=F32)
        norm = jnp.sum(both * both, axis=0, keepdims=True)
        for i in range(qc):
            sm[q * qc + i, :, k * LANES : (k + 1) * LANES] = norm[:, i * LANES : (i + 1) * LANES]
        target[q * quarter : (q + 1) * quarter, :] = both.T.astype(BF16)

    def pick_piece():
        lane = lax.broadcasted_iota(jnp.int32, (slots, tok), 0).astype(F32)
        pick = jnp.where((lane == slot0) | (lane == slot1), 1.0, 0.0)
        pickt[...] = pick.T.astype(BF16)

    def grad_stores():
        return [
            pltpu.make_async_copy(gg, gg_out.at[0], out_sem.at[0]),
            pltpu.make_async_copy(ug, ug_out.at[0], out_sem.at[1]),
            pltpu.make_async_copy(dg, dg_out.at[0], out_sem.at[2]),
        ]

    def own_scores():
        sc_recv[e] = sc_send[e]

    def ms_copy(o, sender):
        return remote(sm.at[o], sm_recv.at[sender], ms_s.at[o], ms_r.at[sender], at_z(o))

    def hand_copy(i):
        src, dst = ((sc_send, sc_sib), (sm, sm_sib), (sm_fin, sm_fin))[i]
        return remote(src, dst, mx_s.at[i], mx_r.at[i], sibling)

    def mg_copy(piece, to):
        return remote(sm_fin.at[piece], sm_fin.at[piece], mg_s.at[to], mg_r.at[piece], at_z(to))

    score_rows = tok // LANES

    def clear_scores():
        sm[:, :, 2 * LANES :] = jnp.zeros((n_z, 1, LANES), F32)

    def small_start():
        own_scores()

        @pl.loop(1, n_ep)
        def _(j):
            s = plane_source(e, j, n_ep)
            sc_copy(s, s).wait_recv()

        got = sc_recv[...].reshape(n_ep, sc_recv.shape[2])
        fill = jnp.zeros((LANES - n_ep, got.shape[1]), F32)
        columns = jnp.concatenate([got, fill], axis=0).T
        totals = [jnp.zeros((1, tok), F32), jnp.zeros((1, tok), F32)]
        lane = lax.broadcasted_iota(jnp.int32, (cap, tok), 0)
        for s in range(n_ep):
            here = (lane + s * cap).astype(F32)
            column = columns[:cap, s : s + 1]
            for k, slot in enumerate((slot0, slot1)):
                totals[k] += jnp.sum(jnp.where(here == slot, column, 0.0), axis=0, keepdims=True)
        clear_scores()
        for k in range(2):
            for h in range(score_rows):
                sm[k * score_rows + h, :, 2 * LANES :] = totals[k][:, h * LANES : (h + 1) * LANES]

        hand_copy(1).wait_recv()
        sm[...] += sm_sib[...]

        @pl.loop(1, n_z)
        def _(j):
            o = (z + j) % n_z
            ms_copy(o, z).start()

    def small_middle():
        @pl.loop(1, n_z)
        def _(j):
            s = (z + j) % n_z
            ms_copy(s, s).wait_recv()

        sm_recv[z] = sm[z]
        sm_fin[z] = jnp.sum(sm_recv[...], axis=0)

        @pl.loop(1, n_z)
        def _(j):
            mg_copy(z, (z + j) % n_z).start()

    def small_end():
        @pl.loop(1, n_z)
        def _(j):
            o = (z + j) % n_z
            mg_copy(o, o).wait_recv()

        hand_copy(2).start()

    def scores(first=0, last=n_ep):
        ones = jnp.ones((8, LANES), F32)
        for b in range(first, last):
            row = lax.dot_general(
                ones, prod[b * cap : (b + 1) * cap, :], CONTRACT_LAST,
                precision=lax.Precision.HIGHEST, preferred_element_type=F32,
            )
            sc_send[b, :, :cap] = row[0:1, :]

    def scores_send():
        hand_copy(0).wait_recv()
        sc_send[...] += sc_sib[...]

        @pl.loop(1, n_ep)
        def _(j):
            p = plane_peer(e, j, n_ep)
            sc_copy(p, e).start()

    def store_start():
        for copy in grad_stores():
            copy.start()

    work = []
    work += [functools.partial(turn_piece, hid, hidt), functools.partial(turn_piece, gpu, gput)]
    for q in range(4):
        work += [functools.partial(down_piece, q)]
        work += [functools.partial(in_piece, 0, q), functools.partial(in_piece, 1, q)]
    work += [store_start]

    sub = slots // SUM_PIECES

    def part(h):
        return pl.ds(h * sub, sub)

    def rd_copy(t, h):
        return remote(
            dn_send.at[t, part(h), :], dn_recv.at[t, part(h), :],
            rd_s.at[t, h], rd_r.at[t, h], at_z(dn_z),
        )

    def ru_copy(t, h):
        return remote(
            up_send.at[t, part(h), :], up_recv.at[t, part(h), :],
            ru_s.at[t, h], ru_r.at[t, h], at_z(up_z),
        )

    def chip_sum(o, h):
        return own[o, part(h), :] + sib_recv[o, part(h), :].astype(F32)

    @pl.when(c != CHAIN_CORE)
    def _():
        for step in [scores, scores_send] + work + [small_start, small_middle, small_end]:
            step()

    @pl.when(c == CHAIN_CORE)
    def _():
        pieces = [functools.partial(scores, b, b + 2) for b in range(0, n_ep, 2)]
        todo = pieces + [hand_copy(0).start] + work + [clear_scores, hand_copy(1).start, pick_piece]
        for t in range(nd):
            o_dn, o_up = (z + n_z - nd + t) % n_z, (z + nu - t + n_z) % n_z
            pt_copy(o_dn).wait_recv()
            pt_copy(o_up).wait_recv()
            for h in range(SUM_PIECES):
                total = chip_sum(o_dn, h)
                if t > 0:
                    rd_copy(t - 1, h).wait_recv()
                    total += dn_recv[t - 1, part(h), :].astype(F32)
                dn_send[t, part(h), :] = total.astype(BF16)
                rd_copy(t, h).start()
                if t < nu:
                    total = chip_sum(o_up, h)
                    if t > 0:
                        ru_copy(t - 1, h).wait_recv()
                        total += up_recv[t - 1, part(h), :].astype(F32)
                    up_send[t, part(h), :] = total.astype(BF16)
                    ru_copy(t, h).start()
                for _ in range(min(t, 1) if n_z == 16 else len(todo)):
                    if todo:
                        todo.pop(0)()

        for h in range(SUM_PIECES):
            total = chip_sum(z, h)
            ru_copy(nu - 1, h).wait_recv()
            total += up_recv[nu - 1, part(h), :].astype(F32)
            rd_copy(nd - 1, h).wait_recv()
            total += dn_recv[nd - 1, part(h), :].astype(F32)
            fin[part(h), :] = total.astype(BF16)

    def fa_copy(b, sender):
        return remote(
            fin.at[block(b), :], gat.at[block(sender), :], fa_s.at[b], fa_r.at[sender], (b, tp)
        )

    def fa_local():
        return pltpu.make_async_copy(fin.at[block(e), :], gat.at[block(e), :], loc_sem.at[1])

    piece = tok // GATHER_PIECES

    def chunk(o, h):
        return tg.at[pl.ds(h * piece, piece), pl.ds(pl.multiple_of(o * LANES, LANES), LANES)]

    def au_copy(t, h, o):
        ref = chunk(o, h)
        hop = 1 if t == 1 else STRIDE
        return remote(ref, ref, au_s.at[t, h], au_r.at[t, h], at_z((z + hop) % n_z))

    def ad_copy(t, h, o):
        ref = chunk(o, h)
        hop = 1 if t == 1 else STRIDE
        return remote(ref, ref, ad_s.at[t, h], ad_r.at[t, h], at_z((z + n_z - hop) % n_z))

    def as_copy(o, h):
        ref = chunk(o, h)
        return remote(ref, ref, as_s.at[o, h], as_r.at[o, h], sibling)

    def store(o):
        at = pl.ds(pl.multiple_of(o * LANES, LANES), LANES)
        return pltpu.make_async_copy(tg.at[:, at], tg_out.at[:, at], out_sem.at[3])

    @pl.when(c == CHAIN_CORE)
    def _():
        fa_local().start()

        @pl.loop(1, n_ep)
        def _(j):
            fa_copy(plane_peer(e, j, n_ep), e).start()

        fa_local().wait()

        @pl.loop(1, n_ep)
        def _(j):
            s = plane_source(e, j, n_ep)
            fa_copy(s, s).wait_recv()

        for h in range(GATHER_PIECES):
            at = slice(h * piece, (h + 1) * piece)
            acc = jnp.dot(pickt[at, :], gat[...], preferred_element_type=F32)
            tg[at, pl.ds(pl.multiple_of(z * LANES, LANES), LANES)] = acc.astype(BF16)
            for t in range(1, STRIDE + 1):
                if t <= nu:
                    au_copy(t, h, z).start()
                ad_copy(t, h, z).start()
            as_copy(z, h).start()
        store(z).start()
        for t in range(1, nd + 1):
            for h in range(GATHER_PIECES):
                if t <= nu:
                    o = (z + n_z - t) % n_z
                    au_copy(t, h, o).wait_recv()
                    if t + STRIDE <= nu:
                        au_copy(t + STRIDE, h, o).start()
                    as_copy(o, h).start()
                o = (z + t) % n_z
                ad_copy(t, h, o).wait_recv()
                if t + STRIDE <= nd:
                    ad_copy(t + STRIDE, h, o).start()
                as_copy(o, h).start()
            if t <= nu:
                store((z + n_z - t) % n_z).start()
            store((z + t) % n_z).start()

    @pl.when(c == CHAIN_CORE)
    def _():
        hand_copy(2).wait_recv()

    units = float(LANES * 2 * n_z)
    for o in range(n_z):
        gn_out[:, o * LANES : (o + 1) * LANES] = sm_fin[o, :, :LANES] / units
        un_out[:, o * LANES : (o + 1) * LANES] = sm_fin[o, :, LANES : 2 * LANES] / units
    dn_out[...] = lax.dot_general(
        jnp.ones((8, LANES), F32), dnacc[...], CONTRACT_LAST,
        precision=lax.Precision.HIGHEST, preferred_element_type=F32,
    )[0:1, :] / float(LANES * n_z)
    for h in range(score_rows):
        at = slice(h * LANES, (h + 1) * LANES)
        gp = gp_ref[:, at]
        total = jnp.zeros((1, LANES), F32)
        for k in range(2):
            ep = ep_ref[k : k + 1, at]
            score = sm_fin[k * score_rows + h, :, 2 * LANES :] / (gp * ep)
            epg_out[k : k + 1, at] = gp * score
            total += ep * score
        gpg_out[:, at] = total

    @pl.when(c != CHAIN_CORE)
    def _():
        @pl.loop(0, n_z)
        def _(j):
            o = (z + n_z + (j % 2) * j - j // 2) % n_z
            for h in range(GATHER_PIECES):
                as_copy(o, h).wait_recv()
            store(o).start()

    for copy in grad_stores():
        copy.wait()

    @pl.loop(1, n_ep)
    def _(j):
        p = plane_peer(e, j, n_ep)
        in_copy(p, p, e).wait_send()

    @pl.loop(0, n_ep)
    def _(s):
        za_copy(s, mine).wait_send()
        zb_copy(s, mine).wait_send()
        dx_copy(s, c).wait_send()
        dy_copy(s, c).wait_send()

    @pl.when(c != CHAIN_CORE)
    def _():
        @pl.loop(1, n_ep)
        def _(j):
            sc_copy(plane_peer(e, j, n_ep), e).wait_send()

        @pl.loop(1, n_z)
        def _(j):
            o = (z + j) % n_z
            ms_copy(o, z).wait_send()
            mg_copy(z, o).wait_send()

        hand_copy(2).wait_send()

        @pl.loop(0, n_z)
        def _(o):
            pt_copy(o).wait_send()

    @pl.when(c == CHAIN_CORE)
    def _():
        hand_copy(0).wait_send()
        hand_copy(1).wait_send()

        @pl.loop(1, n_ep)
        def _(j):
            fa_copy(plane_peer(e, j, n_ep), e).wait_send()

        for h in range(SUM_PIECES):
            for t in range(nd):
                rd_copy(t, h).wait_send()
            for t in range(nu):
                ru_copy(t, h).wait_send()

    @pl.when(c == CHAIN_CORE)
    def _():
        for h in range(GATHER_PIECES):
            for t in range(1, nu + 1):
                au_copy(t, h, z).wait_send()
            for t in range(1, nd + 1):
                ad_copy(t, h, z).wait_send()

            @pl.loop(0, n_z)
            def _(o):
                as_copy(o, h).wait_send()

    pltpu.make_async_copy(tg, tg_out, out_sem.at[3]).wait()


def flush(count, *refs):
    ins, outs, bufs = refs[:count], refs[count : 2 * count], refs[2 * count : 3 * count]
    in_sem, out_sem = refs[3 * count :]
    reads, writes = [], []
    for i in range(count):
        rows = ins[i].shape[-2]
        pieces = 4 if rows % 64 == 0 else 1
        for p in range(pieces):
            at = pl.ds(p * (rows // pieces), rows // pieces)
            src, buf, dst = (
                (ref.at[at, :] if len(ref.shape) == 2 else ref.at[:, at, :])
                for ref in (ins[i], bufs[i], outs[i])
            )
            reads.append(pltpu.make_async_copy(src, buf, in_sem.at[i, p]))
            writes.append(pltpu.make_async_copy(buf, dst, out_sem.at[i, p]))
    for copy in reads:
        copy.start()
    for read, write in zip(reads, writes):
        read.wait()
        write.start()
    for copy in writes:
        copy.wait()


def write_out(arrays):
    count = len(arrays)
    any_spec = pl.BlockSpec(memory_space=pl.ANY)
    return pl.pallas_call(
        functools.partial(flush, count),
        out_shape=tuple(jax.ShapeDtypeStruct(a.shape, a.dtype) for a in arrays),
        in_specs=[any_spec] * count,
        out_specs=(any_spec,) * count,
        scratch_shapes=[pltpu.VMEM(a.shape, a.dtype) for a in arrays]
        + [pltpu.SemaphoreType.DMA((count, 4)), pltpu.SemaphoreType.DMA((count, 4))],
    )(*arrays)


def local(tokens, cotangent, group_prob, expert_prob, routing, gate_weight, up_weight, down_weight):
    tok, width = tokens.shape
    n_ep = lax.axis_size("ep")
    n_z = lax.axis_size("tp") // 2
    cap = 3 * tok * 2 // (2 * n_ep)
    slots = n_ep * cap
    quarter = width // 4
    unit = gate_weight.shape[2]
    nd, nu = n_z // 2, n_z // 2 - 1
    scw = -(-cap // LANES) * LANES
    dma = pltpu.SemaphoreType.DMA
    vm = pltpu.VMEM
    any_spec = pl.BlockSpec(memory_space=pl.ANY)
    vm_spec = pl.BlockSpec(memory_space=pltpu.VMEM)
    outs = pl.pallas_call(
        functools.partial(body, n_ep, n_z, cap),
        out_shape=(
            jax.ShapeDtypeStruct((tok, width), BF16),
            jax.ShapeDtypeStruct((1, width, unit), BF16),
            jax.ShapeDtypeStruct((1, width, unit), BF16),
            jax.ShapeDtypeStruct((1, unit, width), BF16),
            jax.ShapeDtypeStruct((1, width), F32),
            jax.ShapeDtypeStruct((1, width), F32),
            jax.ShapeDtypeStruct((1, unit), F32),
            jax.ShapeDtypeStruct((2, tok), F32),
            jax.ShapeDtypeStruct((1, tok), F32),
        ),
        in_specs=[vm_spec] * 3 + [any_spec] * 5,
        out_specs=(any_spec,) * 4 + (vm_spec,) * 5,
        scratch_shapes=[
            vm((tok, 2 * quarter), BF16),
            vm((2, slots, quarter), BF16),
            vm((2, 4, slots, quarter), BF16),
            vm((4, quarter, 2 * unit), BF16),
            vm((4, unit, quarter), BF16),
            vm((slots, 2 * unit), F32),
            vm((slots, unit), F32),
            vm((slots, 2 * unit), BF16),
            vm((2 * unit, slots), BF16),
            vm((unit, slots), BF16),
            vm((slots, unit), F32),
            vm((n_z, slots, LANES), F32),
            vm((n_z, slots, LANES), BF16),
            vm((n_z, slots, LANES), BF16),
            vm((nd, slots, LANES), BF16),
            vm((nd, slots, LANES), BF16),
            vm((nu, slots, LANES), BF16),
            vm((nu, slots, LANES), BF16),
            vm((n_ep, 1, scw), F32),
            vm((n_ep, 1, scw), F32),
            vm((n_z, 1, 3 * LANES), F32),
            vm((n_z, 1, 3 * LANES), F32),
            vm((n_ep, 1, scw), F32),
            vm((n_z, 1, 3 * LANES), F32),
            vm((n_z, 1, 3 * LANES), F32),
            vm((slots, LANES), BF16),
            vm((slots, LANES), BF16),
            vm((tok, width), BF16),
            vm((width, unit), BF16),
            vm((width, unit), BF16),
            vm((unit, width), BF16),
            vm((unit, LANES), F32),
            dma, dma((4, 3)), dma((2,)),
            dma((n_ep,)), dma((n_ep,)), dma((n_ep,)), dma((n_ep,)), dma((n_ep,)), dma((n_ep,)),
            dma((n_ep,)), dma((n_ep,)), dma((n_ep,)), dma((n_ep,)),
            dma((n_ep,)), dma((n_ep,)),
            dma((n_z,)), dma((n_z,)),
            dma((nd, SUM_PIECES)), dma((nd, SUM_PIECES)), dma((nu, SUM_PIECES)), dma((nu, SUM_PIECES)),
            dma((n_z,)), dma((n_z,)), dma((3,)), dma((3,)), dma((n_z,)), dma((n_z,)),
            dma((n_ep,)), dma((n_ep,)),
            dma((nu + 1, GATHER_PIECES)), dma((nu + 1, GATHER_PIECES)),
            dma((nd + 1, GATHER_PIECES)), dma((nd + 1, GATHER_PIECES)),
            dma((n_z, GATHER_PIECES)), dma((n_z, GATHER_PIECES)),
            dma((4,)), pltpu.SemaphoreType.REGULAR, pltpu.SemaphoreType.REGULAR,
            vm((tok, slots), BF16),
            vm((slots, unit), BF16),
        ],
        compiler_params=pltpu.CompilerParams(
            collective_id=0, has_side_effects=True, vmem_limit_bytes=56 * 1024 * 1024
        ),
    )(
        routing.T, group_prob[None, :], expert_prob.T, tokens, cotangent,
        gate_weight, up_weight, down_weight,
    )
    tg, gg, ug, dg, gn, un, dn, epg, gpg = write_out(outs)
    return tg, gpg[0], epg.T, gg, ug, dg, gn, un, dn


def solution(mesh):
    return jax.shard_map(
        local,
        mesh=mesh,
        in_specs=(
            P("ep", None),
            P("ep", None),
            P("ep"),
            P("ep", None),
            P("ep", None),
            P("ep", None, "tp"),
            P("ep", None, "tp"),
            P("ep", "tp", None),
        ),
        out_specs=(
            P("ep", None),
            P("ep"),
            P("ep", None),
            P("ep", None, "tp"),
            P("ep", None, "tp"),
            P("ep", "tp", None),
            P("ep", None),
            P("ep", None),
            P("ep", "tp"),
        ),
        check_vma=False,
    )
```
